512 devices in a mesh: grp: 2 (over y), sp: 32 (over z), tp: 8 (over x, core).
Axes of the slice: x: 4, y: 2, z: 32, core: 2. Of those that a mesh axis runs over, the one named last changes fastest.
The devices are a block of a 4x8x32 slice.
Arguments:
- layer_input: bfloat16 [4, 16384, 2048], P('grp', 'sp'), parts along dimension 0, may hold values from -6 to 6
- key_weight: bfloat16 [2048, 1024], P(None, 'tp'), may hold values from -0.125 to 0.125
- value_weight: bfloat16 [2048, 1024], P(None, 'tp'), may hold values from -0.125 to 0.125
- beta_weight: bfloat16 [2048, 8], replicated, may hold values from -0.125 to 0.125
- beta_shift: float32 [8], replicated
- decay_weight: bfloat16 [2048, 8], replicated, may hold values from -0.125 to 0.125
- decay_rate: float32 [8], replicated, may hold values from 0 to 0.05
- decay_extra: float32 [4, 16384, 8], P('grp', 'sp', 'tp'), parts along dimension 0, may hold values from -1.5 to 0
- query_new: bfloat16 [4, 1024], P('grp', 'tp'), parts along dimension 0, may hold values from -6 to 6
- gate_new: bfloat16 [4, 1024], P('grp', 'tp'), parts along dimension 0, may hold values from -6 to 6
- norm_gain: float32 [128], replicated, may hold values from 0.1 to 1.9
- out_weight: bfloat16 [8, 128, 2048], P('tp', 'sp'), may hold values from -0.1875 to 0.1875
Outputs:
- state_cache: bfloat16 [4, 8, 128, 128], P('grp', 'tp', None, 'sp'), parts along dimension 0
- read_out: float32 [4, 2048], P('grp', ('sp', 'tp')), parts along dimension 0
The draws below stay inside these ranges and needn't reach their ends.
There are 2 independent parts, one for each index of `grp`. The reference program is written for one: setup_inputs(seed, part) draws one part's arguments, and reference() takes and returns one part's arrays. A program takes and returns all parts, laid end to end along the dimension named above; an argument that names none is the same for every part. Nothing has to cross between parts.
All inputs are finite; a program needn't handle non-finite values.
Results may differ from the reference program's by a relative error of at most 0.013.
Values sent between devices are 32-bit elements; how exact they have to be, the bound alone decides.
A program may use at most 64 MiB of HBM per device.

```python
import math
import jax
import jax.numpy as jnp
from jax import lax

D = 2048
HEAD_TOTAL = 8
DK = 128
BLK = 64
PROMPT_TOTAL = 2
SEG = 512
PROMPT_LENGTH = 16384


def draw_decay_rate(key, part):
    first_key, second_key, third_key = jax.random.split(key, 3)
    head_order = jax.random.permutation(first_key, HEAD_TOTAL)
    slow_count = HEAD_TOTAL // 2
    slow_heads = head_order < slow_count
    fast_rate = jnp.exp(jax.random.uniform(second_key, (HEAD_TOTAL,), jnp.float32, math.log(0.0125), math.log(0.04)))
    slow_rate = jnp.exp(jax.random.uniform(third_key, (HEAD_TOTAL,), jnp.float32, math.log(0.05), math.log(0.2))) / PROMPT_LENGTH
    return jnp.where(slow_heads, slow_rate, fast_rate).astype(jnp.float32)


def draw_beta_shift(key, part):
    first_key = jax.random.fold_in(key, 0)
    head_order = jax.random.permutation(first_key, HEAD_TOTAL)
    slow_count = HEAD_TOTAL // 2
    slow_heads = head_order < slow_count
    fast_key, slow_key = jax.random.split(jax.random.fold_in(key, 7))
    fast_shift = jax.random.uniform(fast_key, (HEAD_TOTAL,), jnp.float32, -1.0, 1.0)
    slow_shift = jax.random.uniform(slow_key, (HEAD_TOTAL,), jnp.float32, math.log(0.06), math.log(0.2)) + math.log(DK / PROMPT_LENGTH)
    return jnp.where(slow_heads, slow_shift, fast_shift).astype(jnp.float32)


def draw_decay_extra(key, part):
    rate_key, position_random_key, length_random_key = jax.random.split(key, 3)
    segments = PROMPT_LENGTH // SEG
    segment_rate = jnp.exp(jax.random.uniform(rate_key, (PROMPT_TOTAL, segments, HEAD_TOTAL), jnp.float32, math.log(0.05), math.log(0.25))) / PROMPT_LENGTH
    drawn_level = jnp.repeat(segment_rate, SEG, axis=1)
    spike_position = jax.random.randint(position_random_key, (PROMPT_TOTAL, 2, HEAD_TOTAL), 0, PROMPT_LENGTH)
    spike_length = jax.random.uniform(length_random_key, (PROMPT_TOTAL, 2, HEAD_TOTAL), jnp.float32, 0.22, 0.5)
    token_positions = jnp.arange(PROMPT_LENGTH)
    spike_marks = (token_positions[None, None, :, None] == spike_position[:, :, None, :]).astype(jnp.float32)
    spike_groups = jnp.sum(spike_marks * spike_length[:, :, None, :], axis=1)
    return (-(drawn_level + spike_groups)).astype(jnp.float32)


def shard_levels(own_key, extent, cuts, low, largest):
    def one(axis_at, parts):
        draws = jax.random.uniform(jax.random.fold_in(jax.random.fold_in(own_key, 6), axis_at), (parts,), jnp.float32, low / len(cuts), largest / len(cuts))
        return jnp.repeat(jnp.exp(draws), extent[axis_at] // parts).reshape((-1,) + (1,) * (len(extent) - axis_at - 1))

    gain = one(*cuts[0])
    for cut in cuts[1:]:
        gain = gain * one(*cut)
    return gain


def centred(key, extent, deviation, most, cuts=(), kind=jnp.bfloat16):
    entries = jax.random.normal(key, extent, jnp.float32) * deviation
    if len(cuts) > 0:
        entries = shard_levels(key, extent, cuts, -0.22, 0.18) * entries
    return jnp.clip(entries, min=-most, max=most).astype(kind)


def setup_inputs(seed: int = 0, part: int = 0) -> dict:
    streams_of = jax.random.split(jax.random.key(seed), 13)
    part_keys = jax.random.split(jax.random.fold_in(streams_of[12], part), 13)
    layer_input = centred(part_keys[0], (PROMPT_TOTAL, PROMPT_LENGTH, D), 1.0, 6.0, ((1, 32),))
    key_weight = centred(streams_of[1], (D, HEAD_TOTAL * DK), D ** -0.5, 0.125, ((1, 8),))
    value_weight = centred(streams_of[2], (D, HEAD_TOTAL * DK), D ** -0.5, 0.125, ((1, 8),))
    beta_weight = centred(streams_of[3], (D, HEAD_TOTAL), D ** -0.5, 0.125)
    beta_shift = draw_beta_shift(jax.random.fold_in(streams_of[12], 71), part)
    decay_weight = centred(streams_of[5], (D, HEAD_TOTAL), D ** -0.5, 0.125)
    decay_rate = draw_decay_rate(jax.random.fold_in(streams_of[12], 71), part)
    decay_extra = draw_decay_extra(jax.random.fold_in(jax.random.fold_in(streams_of[12], part), 71), part)
    query_new = centred(part_keys[8], (PROMPT_TOTAL, HEAD_TOTAL * DK), 1.0, 6.0, ((1, 8),))
    gate_new = centred(part_keys[9], (PROMPT_TOTAL, HEAD_TOTAL * DK), 1.0, 6.0, ((1, 8),))
    norm_gain = jnp.clip(1.0 + 0.18 * jax.random.normal(streams_of[10], (DK,), jnp.float32), 0.1, 1.9)
    out_weight = centred(streams_of[11], (HEAD_TOTAL, DK, D), (HEAD_TOTAL * DK) ** -0.5, 0.1875, ((0, 8), (1, 32)))
    return dict(layer_input=layer_input, key_weight=key_weight, value_weight=value_weight, beta_weight=beta_weight, beta_shift=beta_shift, decay_weight=decay_weight, decay_rate=decay_rate, decay_extra=decay_extra, query_new=query_new, gate_new=gate_new, norm_gain=norm_gain, out_weight=out_weight)


epsilon = 1e-06
highest = lax.Precision.HIGHEST

def chain_states(key_rows, value_rows, beta, log_decay, span):
    seq_here, length, heads_here, head_size = key_rows.shape
    block_count = length // span
    unit_keys = key_rows * lax.rsqrt(lax.optimization_barrier(jnp.sum(key_rows * key_rows, axis=-1, keepdims=True)) + epsilon)

    def blocked(tensor):
        moved_axes = jnp.moveaxis(tensor, 2, 1)
        return moved_axes.reshape((seq_here, heads_here, block_count, span) + tensor.shape[3:])
    key_blocks = blocked(unit_keys)
    value_blocks = blocked(value_rows)
    beta_blocks = blocked(beta)
    cumulative = jnp.cumsum(blocked(log_decay), axis=-1)
    places = jnp.arange(span)
    strict = places[:, None] > places[None, :]
    weighted = key_blocks * beta_blocks[..., None]
    key_products = jnp.einsum('shnid,shnjd->shnij', weighted, key_blocks, precision=highest)
    spread = cumulative[..., :, None] - cumulative[..., None, :]
    lower_part = jnp.where(strict, key_products * jnp.exp(jnp.where(strict, spread, 0.0)), 0.0)
    system = jnp.eye(span, dtype=jnp.float32) + lower_part
    right_side = jnp.concatenate([value_blocks * beta_blocks[..., None], weighted * jnp.exp(cumulative)[..., None]], axis=-1)
    solved = jax.scipy.linalg.solve_triangular(system, right_side, lower=True)
    value_part = solved[..., :head_size]
    key_part = solved[..., head_size:]
    carried_keys = key_blocks * jnp.exp(cumulative[..., -1:] - cumulative)[..., None]
    block_decay = jnp.exp(cumulative[..., -1])
    sequence_in = tuple((jnp.moveaxis(tensor, 2, 0) for tensor in (value_part, key_part, carried_keys, block_decay)))

    def advance(carry_state, inputs):
        value_now, key_now, carried_now, decay_now = inputs
        fresh_values = value_now - jnp.einsum('shck,shkv->shcv', key_now, carry_state, precision=highest)
        carry_state = carry_state * decay_now[..., None, None] + jnp.einsum('shck,shcv->shkv', carried_now, fresh_values, precision=highest)
        return (carry_state, None)
    initial = jnp.zeros((seq_here, heads_here, head_size, head_size), jnp.float32)
    final_state, unused = lax.scan(advance, initial, sequence_in)
    return final_state

def reference(layer_input, key_weight, value_weight, beta_weight, beta_shift, decay_weight, decay_rate, decay_extra, query_new, gate_new, norm_gain, out_weight):
    seq_count, length, width = layer_input.shape
    key_rows = jnp.dot(layer_input.astype(jnp.float32), key_weight.astype(jnp.float32), preferred_element_type=jnp.float32).astype(jnp.bfloat16)
    value_rows = jnp.dot(layer_input.astype(jnp.float32), value_weight.astype(jnp.float32), preferred_element_type=jnp.float32).astype(jnp.bfloat16)
    beta_raw = jnp.dot(layer_input.astype(jnp.float32), beta_weight.astype(jnp.float32), preferred_element_type=jnp.float32).astype(jnp.bfloat16)
    decay_raw = jnp.dot(layer_input.astype(jnp.float32), decay_weight.astype(jnp.float32), preferred_element_type=jnp.float32).astype(jnp.bfloat16)
    beta = jax.nn.sigmoid(beta_raw.astype(jnp.float32) + beta_shift)
    log_decay = -decay_rate * jax.nn.softplus(decay_raw.astype(jnp.float32)) + decay_extra
    key_heads = key_rows.reshape(seq_count, length, HEAD_TOTAL, DK).astype(jnp.float32)
    value_heads = value_rows.reshape(seq_count, length, HEAD_TOTAL, DK).astype(jnp.float32)
    final_state = chain_states(key_heads, value_heads, beta, log_decay, BLK)
    state_cache = final_state.astype(jnp.bfloat16)
    query = query_new.reshape(seq_count, HEAD_TOTAL, DK).astype(jnp.float32)
    query = query * lax.rsqrt(lax.optimization_barrier(jnp.sum(query * query, axis=-1, keepdims=True)) + epsilon) * DK ** (-0.5)
    readout = jnp.einsum('shkv,shk->shv', final_state, query, precision=highest)
    scaled = readout * lax.rsqrt(lax.optimization_barrier(jnp.mean(readout * readout, axis=-1, keepdims=True)) + epsilon)
    gate_values = gate_new.reshape(seq_count, HEAD_TOTAL, DK).astype(jnp.float32)
    normed = (scaled * norm_gain * jax.nn.silu(gate_values)).astype(jnp.bfloat16)
    total = jnp.dot(normed.reshape(seq_count, HEAD_TOTAL * DK).astype(jnp.float32), out_weight.reshape(HEAD_TOTAL * DK, width).astype(jnp.float32), preferred_element_type=jnp.float32)
    return (state_cache, total)
```

```python
import functools

import jax
import jax.numpy as jnp
from jax import lax
from jax.experimental import pallas as pl
from jax.experimental.pallas import tpu as pltpu
from jax.sharding import PartitionSpec as P

MESH = pl.DeviceIdType.MESH
EPS = 1e-06
F32 = jnp.float32
BF16 = jnp.bfloat16
DK = 128
BLK = 128
CH = 32
HALF = DK // CH
NCH = 2 * HALF
QUAD = 4
NT = (((1,), (1,)), ((), ()))


def dot(a, b):
    return jnp.dot(a, b, preferred_element_type=F32)


def split(a):
    high = a.astype(BF16)
    return high, (a - high.astype(F32)).astype(BF16)


def left3(a):
    high, low = split(a)
    return jnp.concatenate([high, low, high], axis=1)


def right3(b):
    high, low = split(b)
    return jnp.concatenate([high, high, low], axis=0)


def left2(a):
    return jnp.concatenate(split(a), axis=1)


def dot3(a, b):
    return dot(left3(a), right3(b))


def local_body(x_hbm, wk_hbm, wv_hbm, bw_ref, dw_ref, shift_ref, rate_ref, extra_ref, ab_ref, w_buf, x_buf, kv_buf, m_buf, t_buf, y_buf, x_sem, w_sem):
    tp = lax.axis_index("tp")
    prompts, seg, width = x_hbm.shape
    rows = 256
    per = seg // rows
    chunks = prompts * per
    copies = []
    wcopies = [
        pltpu.make_async_copy(wk_hbm, w_buf.at[:, pl.ds(0, DK)], w_sem.at[0]),
        pltpu.make_async_copy(wv_hbm, w_buf.at[:, pl.ds(DK, DK)], w_sem.at[1]),
    ]
    for c in wcopies:
        c.start()
    for j in range(chunks):
        c = pltpu.make_async_copy(
            x_hbm.at[j // per, pl.ds((j % per) * rows, rows), :], x_buf.at[pl.ds(j * rows, rows), :], x_sem.at[j]
        )
        c.start()
        copies.append(c)
    wbd = jnp.concatenate([bw_ref[...], dw_ref[...]], axis=0)
    for c in wcopies:
        c.wait()
    raw = []
    for j in range(chunks):
        copies[j].wait()
        xs = x_buf[pl.ds(j * rows, rows), :]
        kv_buf[pl.ds(j * rows, rows), :] = dot(xs, w_buf[...]).astype(BF16)
        raw.append(lax.dot_general(wbd, xs, NT, preferred_element_type=F32))
    groups = prompts * seg // BLK
    gp = seg // BLK
    heads = bw_ref.shape[0]
    head_lane = lax.broadcasted_iota(jnp.int32, (2 * heads, 1), 0)
    pick_b = head_lane == tp
    pick_d = head_lane == tp + heads

    def pack(pick):
        lines = []
        for g in range(groups):
            at = g * BLK
            block = raw[at // rows][:, at % rows : at % rows + BLK]
            lines.append(jnp.sum(jnp.where(pick, block, 0.0), axis=0, keepdims=True))
        return jnp.concatenate(lines, axis=0)

    beta_raw = pack(pick_b).astype(BF16).astype(F32)
    decay_raw = pack(pick_d).astype(BF16).astype(F32)
    extra = jnp.concatenate(
        [extra_ref[g // gp, :, pl.ds((g % gp) * BLK, BLK)] for g in range(groups)], axis=0
    )
    beta = jax.nn.sigmoid(beta_raw + shift_ref[tp])
    softplus = jnp.maximum(decay_raw, 0.0) + jnp.log1p(jnp.exp(-jnp.abs(decay_raw)))
    log_decay = -rate_ref[tp] * softplus + extra
    row = lax.broadcasted_iota(jnp.int32, (BLK, BLK), 0)
    col = lax.broadcasted_iota(jnp.int32, (BLK, BLK), 1)
    upto = jnp.where(row <= col, 1.0, 0.0).astype(BF16)
    l1 = log_decay.astype(BF16)
    l2 = (log_decay - l1.astype(F32)).astype(BF16)
    l3 = (log_decay - l1.astype(F32) - l2.astype(F32)).astype(BF16)
    cum = dot(jnp.concatenate([l1, l2, l3], axis=1), jnp.concatenate([upto, upto, upto], axis=0))
    cum_t = cum.T
    beta_t = beta.T
    eye = row == col
    upper = row < col
    ident = jnp.where(eye, 1.0, 0.0)
    neu = upper & ((row >> 3) == (col >> 3))
    norms = []
    for g in range(groups):
        k = kv_buf[pl.ds(g * BLK, BLK), pl.ds(0, DK)]
        gram = lax.dot_general(k, k, NT, preferred_element_type=F32)
        diag = jnp.where(eye, gram, 0.0)
        r_row = lax.rsqrt(jnp.sum(diag, axis=0, keepdims=True) + EPS)
        r_col = lax.rsqrt(jnp.sum(diag, axis=1, keepdims=True) + EPS)
        c_row = cum[g : g + 1, :]
        c_col = cum_t[:, g : g + 1]
        scale = jnp.exp(jnp.where(upper, c_row - c_col, 0.0)) * (beta[g : g + 1, :] * r_row) * r_col
        m = jnp.where(upper, gram * scale, 0.0)
        m_buf[g] = m
        t_buf[g] = jnp.where(neu, m, 0.0)
        norms.append((r_row, r_col))
    p2 = []
    for g in range(groups):
        p = t_buf[g]
        p2.append(dot3(p, p))
    for g in range(groups):
        p = t_buf[g]
        both = dot3(p2[g], jnp.concatenate([p2[g], p], axis=1))
        y_buf[g] = both[:, :BLK]
        t_buf[g] = ident - p + p2[g] - both[:, BLK:]
    for g in range(groups):
        q = t_buf[g]
        t_buf[g] = q + dot3(q, y_buf[g])
    s = 8
    while s < BLK:
        mask = ((row // (2 * s)) == (col // (2 * s))) & ((row // s) % 2 == 0) & ((col // s) % 2 == 1)
        for g in range(groups):
            y_buf[g] = dot3(jnp.where(mask, m_buf[g], 0.0), t_buf[g])
        for g in range(groups):
            t = t_buf[g]
            t_buf[g] = t - dot3(t, y_buf[g])
        s *= 2
    for g in range(groups):
        r_row, r_col = norms[g]
        c_row = cum[g : g + 1, :]
        last = cum[g : g + 1, BLK - 1 : BLK]
        t = t_buf[g] * (jnp.exp(last - c_row) * r_row)
        b_col = beta_t[:, g : g + 1]
        e_col = jnp.exp(cum_t[:, g : g + 1]) * r_col * b_col
        k = kv_buf[pl.ds(g * BLK, BLK), pl.ds(0, DK)]
        v = kv_buf[pl.ds(g * BLK, BLK), pl.ds(DK, DK)]
        k2 = jnp.concatenate([k, k], axis=0)
        f = dot(left2(jnp.concatenate([t * e_col, t * b_col], axis=0)), k2)
        kt = k.T
        vt = v.T
        a_part = dot(jnp.concatenate([kt, kt], axis=1), jnp.concatenate(split(f[:BLK]), axis=0))
        b_part = dot(jnp.concatenate([vt, vt], axis=1), jnp.concatenate(split(f[BLK:]), axis=0))
        y_buf2 = jnp.concatenate([ident * jnp.exp(last) - a_part, b_part], axis=0)
        if g % gp == 0:
            maps = []
        maps.append(y_buf2)
        if g % gp == gp - 1:
            while len(maps) > 1:
                nexts = []
                for a in range(0, len(maps), 2):
                    early, late = maps[a], maps[a + 1]
                    prod = dot3(early, late[:DK])
                    nexts.append(jnp.concatenate([prod[:DK], prod[DK:] + late[DK:]], axis=0))
                maps = nexts
            p = g // gp
            for c in range(NCH):
                ab_ref[c, p] = maps[0][c * CH : (c + 1) * CH]


def comm_body(n, ntp, first_quad, ab_ref, q_ref, gate_ref, gain_ref, ow_ref, st_ref, ro_ref, lc_in, pc_in, lc_out, pc_out, comp, rhs, rhs2, b0_in, s_buf, st_in, nm_out, nm_in, ow_out, ow_all, ow_mat, part, tot, fin_in, lc_ss, lc_rs, pc_ss, pc_rs, b0_ss, b0_rs, st_ss, st_rs, nm_ss, nm_rs, ow_ss, ow_rs, pt_ss, pt_rs, fn_ss, fn_rs, rdy_lc, rdy_pc, rdy_b0):
    grp = lax.axis_index("grp")
    z = lax.axis_index("sp")
    tp = lax.axis_index("tp")
    last = n - 1
    prompts = ab_ref.shape[1]
    tiles = tot.shape[0]

    def dev(zz, t=None):
        return (grp, zz, tp if t is None else t)

    in_quad = z >= first_quad
    pos = lax.rem(jnp.maximum(z - first_quad, 0), QUAD)
    lc_recv = in_quad & (pos > 0)
    lc_send = in_quad & (pos < QUAD - 1)
    head = (z >= 1) & ((z < first_quad) | (in_quad & (pos == QUAD - 1)))
    pc_recv = head & (z > 1)
    pc_send = head & (z < last)
    prev_head = jnp.where(z <= first_quad - 1, z - 1, z - QUAD)
    next_head = jnp.where(z < first_quad - 1, z + 1, z + QUAD)

    bar = pltpu.get_barrier_semaphore()

    @pl.when(z == 1)
    def _():
        for zz in range(n):
            if zz != 1:
                pl.semaphore_signal(bar, inc=1, device_id=dev(zz), device_id_type=MESH)
        for k in range(1, ntp):
            pl.semaphore_signal(bar, inc=1, device_id=dev(z, lax.rem(tp + k, ntp)), device_id_type=MESH)

    @pl.when(lc_send)
    def _():
        pl.semaphore_signal(bar, inc=1, device_id=dev(z + 1), device_id_type=MESH)

    @pl.when(pc_send)
    def _():
        pl.semaphore_signal(bar, inc=1, device_id=dev(next_head), device_id_type=MESH)

    @pl.when(z != last)
    def _():
        pl.semaphore_signal(bar, inc=1, device_id=dev(last), device_id_type=MESH)

    one = jnp.int32(1)
    zero = jnp.int32(0)
    expect = (
        jnp.where(z == 1, ntp - 1, 1)
        + jnp.where(lc_recv, one, zero)
        + jnp.where(pc_recv, one, zero)
        + jnp.where(z == last, n - 1, 0)
    )
    pl.semaphore_wait(bar, expect)

    @pl.when(lc_recv)
    def _():
        pl.semaphore_signal(rdy_lc, inc=1, device_id=dev(z - 1), device_id_type=MESH)

    @pl.when(pc_recv)
    def _():
        pl.semaphore_signal(rdy_pc, inc=1, device_id=dev(prev_head), device_id_type=MESH)

    @pl.when(z == last)
    def _():
        pl.semaphore_signal(rdy_b0, inc=1, device_id=dev(0), device_id_type=MESH)

    ow = ow_ref[0].astype(F32)

    def ow_copy():
        return pltpu.make_async_remote_copy(
            src_ref=ow_out, dst_ref=ow_all.at[z], send_sem=ow_ss, recv_sem=ow_rs.at[z], device_id=dev(1), device_id_type=MESH
        )

    @pl.when(z != 1)
    def _():
        ow_out[...] = ow
        ow_copy().start()

    @pl.when(z == 1)
    def _():
        ow_all[1] = ow

    def lc_copy(src, c):
        return pltpu.make_async_remote_copy(
            src_ref=src.at[c], dst_ref=lc_in.at[c], send_sem=lc_ss.at[c], recv_sem=lc_rs.at[c], device_id=dev(z + 1), device_id_type=MESH
        )

    def pc_copy(src, c):
        return pltpu.make_async_remote_copy(
            src_ref=src.at[c], dst_ref=pc_in.at[c], send_sem=pc_ss.at[c], recv_sem=pc_rs.at[c], device_id=dev(next_head), device_id_type=MESH
        )

    def b0_copy(c):
        return pltpu.make_async_remote_copy(
            src_ref=ab_ref.at[HALF + c], dst_ref=b0_in.at[c], send_sem=b0_ss.at[c], recv_sem=b0_rs.at[c], device_id=dev(last), device_id_type=MESH
        )

    def set_rhs(dst, src):
        for p in range(prompts):
            a = jnp.concatenate([src[c, p] for c in range(HALF)], axis=0)
            dst[p] = right3(a)

    @pl.when(lc_recv)
    def _():
        set_rhs(rhs, ab_ref)

        @pl.when(lc_send)
        def _():
            pl.semaphore_wait(rdy_lc, 1)

        def step(c, carry):
            lc_copy(ab_ref, c).wait_recv()
            for p in range(prompts):
                y = dot(left3(lc_in[c, p]), rhs[p])
                y = y + jnp.where(c >= HALF, ab_ref[c, p], 0.0)
                lc_out[c, p] = y
                comp[c, p] = y

            @pl.when(lc_send)
            def _():
                lc_copy(lc_out, c).start()

            return carry

        lax.fori_loop(0, NCH, step, 0)

    @pl.when(lc_send & (pos == 0))
    def _():
        pl.semaphore_wait(rdy_lc, 1)
        for c in range(NCH):
            lc_copy(ab_ref, c).start()

    @pl.when((z == 1) & pc_send)
    def _():
        pl.semaphore_wait(rdy_pc, 1)
        for c in range(NCH):
            pc_copy(ab_ref, c).start()

    @pl.when(z == 0)
    def _():
        pl.semaphore_wait(rdy_b0, 1)
        for c in range(HALF):
            b0_copy(c).start()

    @pl.when(pc_recv)
    def _():
        @pl.when(jnp.logical_not(lc_recv))
        def _():
            for c in range(NCH):
                comp[c] = ab_ref[c]

        set_rhs(rhs2, comp)

        @pl.when(pc_send)
        def _():
            pl.semaphore_wait(rdy_pc, 1)

        def step(c, carry):
            pc_copy(ab_ref, c).wait_recv()
            for p in range(prompts):
                y = dot(left3(pc_in[c, p]), rhs2[p])
                pc_out[c, p] = y + jnp.where(c >= HALF, comp[c, p], 0.0)

            @pl.when(pc_send)
            def _():
                pc_copy(pc_out, c).start()

            return carry

        lax.fori_loop(0, NCH, step, 0)

    def st_copy(zz):
        t = zz // 2
        per = CH // 8
        return pltpu.make_async_remote_copy(
            src_ref=s_buf.at[t // per, :, pl.ds((t % per) * 8, 8), :], dst_ref=st_in, send_sem=st_ss.at[zz], recv_sem=st_rs, device_id=dev(zz), device_id_type=MESH
        )

    def nm_copy():
        return pltpu.make_async_remote_copy(
            src_ref=nm_out, dst_ref=nm_in, send_sem=nm_ss, recv_sem=nm_rs, device_id=dev(1), device_id_type=MESH
        )

    order = []
    for k in range(n):
        for zz in (k, last - 1 - k):
            if zz not in order and 0 <= zz < last:
                order.append(zz)

    @pl.when(z == last)
    def _():
        set_rhs(rhs, pc_out)
        for c in range(HALF):
            b0_copy(c).wait_recv()
        query = q_ref[...].astype(F32)
        query = query * lax.rsqrt(jnp.sum(query * query, axis=-1, keepdims=True) + EPS) * DK**-0.5
        reads = []
        for p in range(prompts):
            start = jnp.concatenate([b0_in[c, p] for c in range(HALF)], axis=0)
            fin = dot(left3(start), rhs[p])
            fin = fin + jnp.concatenate([pc_out[HALF + c, p] for c in range(HALF)], axis=0)
            for c in range(HALF):
                s_buf[c, p] = fin[c * CH : (c + 1) * CH]
            qh, ql = split(jnp.broadcast_to(query[p : p + 1], (8, DK)))
            fh, fl = split(fin)
            read = lax.dot_general(
                jnp.concatenate([qh, ql, qh], axis=1), jnp.concatenate([fh, fh, fl], axis=1), NT, preferred_element_type=F32
            )
            reads.append(read[0:1])
        for zz in order:
            st_copy(zz).start()
        read = jnp.concatenate(reads, axis=0)
        scaled = read * lax.rsqrt(jnp.mean(read * read, axis=-1, keepdims=True) + EPS)
        gate = gate_ref[...].astype(F32)
        normed = (scaled * gain_ref[...] * (gate * jax.nn.sigmoid(gate))).astype(BF16)
        nm_out[...] = normed.astype(F32)
        nm_copy().start()
        t = last // 2
        per = CH // 8
        for p in range(prompts):
            st_in[p] = s_buf[t // per, p, (t % per) * 8 : (t % per) * 8 + 8, :]

    def pt_copy(k):
        return pltpu.make_async_remote_copy(
            src_ref=part.at[tp], dst_ref=part.at[tp], send_sem=pt_ss.at[k], recv_sem=pt_rs.at[k], device_id=dev(1, lax.rem(tp + k, ntp)), device_id_type=MESH
        )

    def fin_copy(zz):
        return pltpu.make_async_remote_copy(
            src_ref=tot.at[zz // 2], dst_ref=fin_in, send_sem=fn_ss.at[zz], recv_sem=fn_rs, device_id=dev(zz), device_id_type=MESH
        )

    out_order = [0] + [zz for k in range(1, n) for zz in (1 + k, (1 - k) % n) if zz < n]
    out_order = [zz for i, zz in enumerate(out_order) if zz != 1 and zz not in out_order[:i]]

    @pl.when(z == 1)
    def _():
        for zz in range(n):
            if zz != 1:
                pltpu.make_async_remote_copy(
                    src_ref=ow_out, dst_ref=ow_all.at[zz], send_sem=ow_ss, recv_sem=ow_rs.at[zz], device_id=dev(1), device_id_type=MESH
                ).wait_recv()
        lines = ow_all.shape[1]
        for r in range(lines):
            ow_mat[pl.ds(r * n, n), :] = ow_all[:, r, :].astype(BF16)
        vr = lax.broadcasted_iota(jnp.int32, (DK, DK), 0)
        vc = lax.broadcasted_iota(jnp.int32, (DK, DK), 1)
        perm = jnp.where(vc == (vr % lines) * n + vr // lines, 1.0, 0.0).astype(BF16)
        half = ow_mat.shape[1] // 4
        for h in range(4):
            ow_mat[:, pl.ds(h * half, half)] = dot(perm, ow_mat[:, pl.ds(h * half, half)]).astype(BF16)
        nm_copy().wait_recv()
        lhs = jnp.concatenate([nm_in[...], jnp.zeros((8 - prompts, DK), F32)], axis=0).astype(BF16)
        res = dot(lhs, ow_mat[...])
        for t in range(tiles):
            part[tp, t] = res[0:prompts, t * 128 : (t + 1) * 128]
        for k in range(1, ntp):
            pt_copy(k).start()
        for k in range(1, ntp):
            pltpu.make_async_remote_copy(
                src_ref=part.at[tp], dst_ref=part.at[tp], send_sem=pt_ss.at[k], recv_sem=pt_rs.at[k], device_id=dev(1, lax.rem(tp + k, ntp)), device_id_type=MESH
            ).wait_recv()
        acc = part[0]
        for k in range(1, ntp):
            acc = acc + part[k]
        tot[...] = acc
        for zz in out_order:
            fin_copy(zz).start()
        fin_in[...] = acc[0]

    @pl.when(z != last)
    def _():
        pltpu.make_async_remote_copy(
            src_ref=st_in, dst_ref=st_in, send_sem=st_ss.at[0], recv_sem=st_rs, device_id=dev(last), device_id_type=MESH
        ).wait_recv()

    odd = lax.rem(z, 2)
    for p in range(prompts):
        st_ref[p] = jnp.where(odd == 1, st_in[p, 4:8, :], st_in[p, 0:4, :]).astype(BF16)

    @pl.when(z != 1)
    def _():
        pltpu.make_async_remote_copy(
            src_ref=fin_in, dst_ref=fin_in, send_sem=fn_ss.at[0], recv_sem=fn_rs, device_id=dev(1), device_id_type=MESH
        ).wait_recv()

    span = ro_ref.shape[1]
    first = odd * (ntp * span) + tp * span
    value = fin_in[...]
    lane = lax.broadcasted_iota(jnp.int32, (128, span), 0)
    want = lax.broadcasted_iota(jnp.int32, (128, span), 1) + first
    v1, v2 = split(value)
    v3 = (value - v1.astype(F32) - v2.astype(F32)).astype(BF16)
    sel = jnp.where(lane == want, 1.0, 0.0).astype(BF16)
    ro_ref[...] = dot(v1, sel) + dot(v2, sel) + dot(v3, sel)

    @pl.when(z != 1)
    def _():
        ow_copy().wait_send()

    @pl.when(lc_send)
    def _():
        for c in range(NCH):
            lc_copy(lc_out, c).wait_send()

    @pl.when(pc_send)
    def _():
        for c in range(NCH):
            pc_copy(pc_out, c).wait_send()

    @pl.when(z == 0)
    def _():
        for c in range(HALF):
            b0_copy(c).wait_send()

    @pl.when(z == last)
    def _():
        for zz in range(n):
            if zz != last:
                st_copy(zz).wait_send()
        nm_copy().wait_send()

    @pl.when(z == 1)
    def _():
        for k in range(1, ntp):
            pt_copy(k).wait_send()
        for zz in range(n):
            if zz != 1:
                fin_copy(zz).wait_send()


VM = pl.BlockSpec(memory_space=pltpu.VMEM)
SM = pl.BlockSpec(memory_space=pltpu.SMEM)
ANY = pl.BlockSpec(memory_space=pl.ANY)


def local_map(x, wk, wv, bw, dw, shift, rate, extra):
    prompts, seg, width = x.shape
    total = prompts * seg
    groups = total // BLK
    chunks = total // 256
    return pl.pallas_call(
        local_body,
        name="local_map",
        out_shape=jax.ShapeDtypeStruct((NCH, prompts, CH, DK), F32),
        in_specs=[ANY, ANY, ANY, VM, VM, SM, SM, VM],
        out_specs=VM,
        scratch_shapes=[
            pltpu.VMEM((width, 2 * DK), BF16),
            pltpu.VMEM((total, width), BF16),
            pltpu.VMEM((total, 2 * DK), BF16),
            pltpu.VMEM((groups, BLK, BLK), F32),
            pltpu.VMEM((groups, BLK, BLK), F32),
            pltpu.VMEM((groups, BLK, BLK), F32),
            pltpu.SemaphoreType.DMA((chunks,)),
            pltpu.SemaphoreType.DMA((2,)),
        ],
    )(x, wk, wv, bw, dw, shift, rate, extra)


def exchange(n, ntp, ab, q, gate, gain, ow):
    prompts = ab.shape[1]
    width = ow.shape[2]
    lines = ow.shape[1]
    quads = 3 if n >= 32 else 1
    first_quad = n - QUAD * quads
    span = width // (n * ntp)
    tiles = width // 128
    blk = pltpu.VMEM((NCH, prompts, CH, DK), F32)
    dma = pltpu.SemaphoreType.DMA
    return pl.pallas_call(
        functools.partial(comm_body, n, ntp, first_quad),
        name="exchange",
        out_shape=(
            jax.ShapeDtypeStruct((prompts, lines, DK), BF16),
            jax.ShapeDtypeStruct((prompts, span), F32),
        ),
        in_specs=[VM] * 5,
        out_specs=(VM, VM),
        scratch_shapes=[
            blk, blk, blk, blk, blk,
            pltpu.VMEM((prompts, 3 * DK, DK), BF16),
            pltpu.VMEM((prompts, 3 * DK, DK), BF16),
            pltpu.VMEM((HALF, prompts, CH, DK), F32),
            pltpu.VMEM((HALF, prompts, CH, DK), F32),
            pltpu.VMEM((prompts, 8, DK), F32),
            pltpu.VMEM((prompts, DK), F32),
            pltpu.VMEM((prompts, DK), F32),
            pltpu.VMEM((lines, width), F32),
            pltpu.VMEM((n, lines, width), F32),
            pltpu.VMEM((n * lines, width), BF16),
            pltpu.VMEM((ntp, tiles, prompts, 128), F32),
            pltpu.VMEM((tiles, prompts, 128), F32),
            pltpu.VMEM((prompts, 128), F32),
            dma((NCH,)), dma((NCH,)), dma((NCH,)), dma((NCH,)),
            dma((HALF,)), dma((HALF,)),
            dma((n,)), dma,
            dma, dma,
            dma, dma((n,)),
            dma((ntp,)), dma((ntp,)),
            dma((n,)), dma,
            pltpu.SemaphoreType.REGULAR, pltpu.SemaphoreType.REGULAR, pltpu.SemaphoreType.REGULAR,
        ],
        compiler_params=pltpu.CompilerParams(collective_id=0, has_side_effects=True),
    )(ab, q, gate, gain, ow)


def solution(mesh):
    n, ntp = mesh.shape["sp"], mesh.shape["tp"]

    def per_device(x, wk, wv, bw, shift, dw, rate, extra, q, gate, gain, ow):
        prompts, seg, width = x.shape
        ab = local_map(x, wk, wv, bw.T, dw.T, shift, rate, extra.reshape(prompts, 1, seg))
        st, ro = exchange(n, ntp, ab, q, gate, gain.reshape(1, -1), ow)
        return jnp.transpose(st, (0, 2, 1))[:, None], ro

    placed = (
        P("grp", "sp", None),
        P(None, "tp"),
        P(None, "tp"),
        P(),
        P(),
        P(),
        P(),
        P("grp", "sp", "tp"),
        P("grp", "tp"),
        P("grp", "tp"),
        P(),
        P("tp", "sp", None),
    )
    return jax.shard_map(
        per_device,
        mesh=mesh,
        in_specs=placed,
        out_specs=(P("grp", "tp", None, "sp"), P("grp", ("sp", "tp"))),
        check_vma=False,
    )
```

```python
import functools

import jax
import jax.numpy as jnp
from jax import lax
from jax.experimental import pallas as pl
from jax.experimental.pallas import tpu as pltpu
from jax.sharding import PartitionSpec as P

MESH = pl.DeviceIdType.MESH
EPS = 1e-06
F32 = jnp.float32
BF16 = jnp.bfloat16
DK = 128
BLK = 128
CH = 16
ROWS = 256
HALF = DK // CH
NCH = 2 * HALF
GROUPS = (1, 1, 1, 1, 1, 2, 2, 2, 2, 2, 3, 3, 4, 6)
NT = (((1,), (1,)), ((), ()))


def dot(a, b):
    return jnp.dot(a, b, preferred_element_type=F32)


def split(a):
    high = a.astype(BF16)
    return high, (a - high.astype(F32)).astype(BF16)


def left3(a):
    high, low = split(a)
    return jnp.concatenate([high, low, high], axis=1)


def right3(b):
    high, low = split(b)
    return jnp.concatenate([high, high, low], axis=0)


def left2(a):
    return jnp.concatenate(split(a), axis=1)


def dot3(a, b):
    return dot(left3(a), right3(b))


def local_body(tp, prompts, seg, wcopies, copies, scopies, bw_ref, dw_ref, shift_ref, rate_ref, extra_ref, ab_ref, w_buf, x_buf, kv_buf, m_buf, t_buf, y_buf):
    rows = ROWS
    chunks = len(copies)
    for c in scopies:
        c.wait()
    wbd = jnp.concatenate([bw_ref[...], dw_ref[...]], axis=0)
    for c in wcopies:
        c.wait()
    raw = []
    for j in range(chunks):
        copies[j].wait()
        xs = x_buf[pl.ds(j * rows, rows), :]
        kv_buf[pl.ds(j * rows, rows), :] = dot(xs, w_buf[...]).astype(BF16)
        raw.append(lax.dot_general(wbd, xs, NT, preferred_element_type=F32))
    groups = prompts * seg // BLK
    gp = seg // BLK
    heads = bw_ref.shape[0]
    head_lane = lax.broadcasted_iota(jnp.int32, (2 * heads, 1), 0)
    pick_b = head_lane == tp
    pick_d = head_lane == tp + heads

    def pack(pick):
        lines = []
        for g in range(groups):
            at = g * BLK
            block = raw[at // rows][:, at % rows : at % rows + BLK]
            lines.append(jnp.sum(jnp.where(pick, block, 0.0), axis=0, keepdims=True))
        return jnp.concatenate(lines, axis=0)

    beta_raw = pack(pick_b).astype(BF16).astype(F32)
    decay_raw = pack(pick_d).astype(BF16).astype(F32)
    extra = jnp.concatenate(
        [extra_ref[g // gp, :, pl.ds((g % gp) * BLK, BLK)] for g in range(groups)], axis=0
    )
    own = lax.broadcasted_iota(jnp.int32, (1, heads), 1) == tp
    shift = jnp.sum(jnp.where(own, shift_ref[...], 0.0), axis=1, keepdims=True)
    rate = jnp.sum(jnp.where(own, rate_ref[...], 0.0), axis=1, keepdims=True)
    beta = jax.nn.sigmoid(beta_raw + shift)
    softplus = jnp.maximum(decay_raw, 0.0) + jnp.log1p(jnp.exp(-jnp.abs(decay_raw)))
    log_decay = -rate * softplus + extra
    row = lax.broadcasted_iota(jnp.int32, (BLK, BLK), 0)
    col = lax.broadcasted_iota(jnp.int32, (BLK, BLK), 1)
    upto = jnp.where(row <= col, 1.0, 0.0).astype(BF16)
    l1 = log_decay.astype(BF16)
    l2 = (log_decay - l1.astype(F32)).astype(BF16)
    l3 = (log_decay - l1.astype(F32) - l2.astype(F32)).astype(BF16)
    cum = dot(jnp.concatenate([l1, l2, l3], axis=1), jnp.concatenate([upto, upto, upto], axis=0))
    cum_t = cum.T
    beta_t = beta.T
    eye = row == col
    upper = row < col
    ident = jnp.where(eye, 1.0, 0.0)
    neu = upper & ((row >> 3) == (col >> 3))
    norms = []
    for g in range(groups):
        k = kv_buf[pl.ds(g * BLK, BLK), pl.ds(0, DK)]
        gram = lax.dot_general(k, k, NT, preferred_element_type=F32)
        diag = jnp.where(eye, gram, 0.0)
        r_row = lax.rsqrt(jnp.sum(diag, axis=0, keepdims=True) + EPS)
        r_col = lax.rsqrt(jnp.sum(diag, axis=1, keepdims=True) + EPS)
        c_row = cum[g : g + 1, :]
        c_col = cum_t[:, g : g + 1]
        scale = jnp.exp(jnp.where(upper, c_row - c_col, 0.0)) * (beta[g : g + 1, :] * r_row) * r_col
        m = jnp.where(upper, gram * scale, 0.0)
        m_buf[g] = m
        t_buf[g] = jnp.where(neu, m, 0.0)
        norms.append((r_row, r_col))
    p2 = []
    for g in range(groups):
        p = t_buf[g]
        p2.append(dot3(p, p))
    for g in range(groups):
        p = t_buf[g]
        both = dot3(p2[g], jnp.concatenate([p2[g], p], axis=1))
        y_buf[g] = both[:, :BLK]
        t_buf[g] = ident - p + p2[g] - both[:, BLK:]
    for g in range(groups):
        q = t_buf[g]
        t_buf[g] = q + dot3(q, y_buf[g])
    s = 8
    while s < BLK:
        mask = ((row // (2 * s)) == (col // (2 * s))) & ((row // s) % 2 == 0) & ((col // s) % 2 == 1)
        for g in range(groups):
            y_buf[g] = dot3(jnp.where(mask, m_buf[g], 0.0), t_buf[g])
        for g in range(groups):
            t = t_buf[g]
            t_buf[g] = t - dot3(t, y_buf[g])
        s *= 2
    for g in range(groups):
        r_row, r_col = norms[g]
        c_row = cum[g : g + 1, :]
        last = cum[g : g + 1, BLK - 1 : BLK]
        t = t_buf[g] * (jnp.exp(last - c_row) * r_row)
        b_col = beta_t[:, g : g + 1]
        e_col = jnp.exp(cum_t[:, g : g + 1]) * r_col * b_col
        k = kv_buf[pl.ds(g * BLK, BLK), pl.ds(0, DK)]
        v = kv_buf[pl.ds(g * BLK, BLK), pl.ds(DK, DK)]
        k2 = jnp.concatenate([k, k], axis=0)
        f = dot(left2(jnp.concatenate([t * e_col, t * b_col], axis=0)), k2)
        kt = k.T
        vt = v.T
        a_part = dot(jnp.concatenate([kt, kt], axis=1), jnp.concatenate(split(f[:BLK]), axis=0))
        b_part = dot(jnp.concatenate([vt, vt], axis=1), jnp.concatenate(split(f[BLK:]), axis=0))
        y_buf2 = jnp.concatenate([ident * jnp.exp(last) - a_part, b_part], axis=0)
        if g % gp == 0:
            maps = []
        maps.append(y_buf2)
        if g % gp == gp - 1:
            while len(maps) > 1:
                nexts = []
                for a in range(0, len(maps), 2):
                    early, late = maps[a], maps[a + 1]
                    prod = dot3(early, late[:DK])
                    nexts.append(jnp.concatenate([prod[:DK], prod[DK:] + late[DK:]], axis=0))
                maps = nexts
            p = g // gp
            for c in range(NCH):
                ab_ref[c, p] = maps[0][c * CH : (c + 1) * CH]


def body(n, ntp, sizes, x_hbm, wk_hbm, wv_hbm, bw_hbm, shift_hbm, dw_hbm, rate_hbm, extra_hbm, q_hbm, gate_hbm, gain_hbm, ow_hbm, st_ref, ro_ref, w_buf, x_buf, kv_buf, m_buf, t_buf, y_buf, bw_ref, shift_ref, dw_ref, rate_ref, extra_ref, q_ref, gate_ref, gain_ref, ow_ref, ab_ref, lc_in, pc_in, lc_out, pc_out, comp, rhs, rhs2, b0_in, dummy, st_in, nm_out, nm_in, ow_out, ow_all, ow_mat, part, part0, tot, fin_in, x_sem, w_sem, in_sem, lc_ss, lc_rs, pc_ss, pc_rs, b0_ss, b0_rs, st_ss, st_rs, nm_ss, nm_rs, ow_ss, ow_rs, pt_ss, pt_rs, p0_ss, p0_rs, fn_ss, fn_rs, rdy_lc, rdy_pc, rdy_b0, rdy_p0):
    grp = lax.axis_index("grp")
    z = lax.axis_index("sp")
    tp = lax.axis_index("tp")
    last = n - 1
    prompts, seg, width = x_hbm.shape
    tiles = tot.shape[0]
    span = ro_ref.shape[1]

    wcopies = [
        pltpu.make_async_copy(wk_hbm, w_buf.at[:, pl.ds(0, DK)], w_sem.at[0]),
        pltpu.make_async_copy(wv_hbm, w_buf.at[:, pl.ds(DK, DK)], w_sem.at[1]),
    ]
    small = [(bw_hbm, bw_ref), (dw_hbm, dw_ref), (shift_hbm, shift_ref), (rate_hbm, rate_ref), (extra_hbm, extra_ref), (q_hbm, q_ref), (gate_hbm, gate_ref), (gain_hbm, gain_ref), (ow_hbm, ow_ref)]
    scopies = [pltpu.make_async_copy(a, b, in_sem.at[i]) for i, (a, b) in enumerate(small)]
    per = seg // ROWS
    copies = []
    for j in range(prompts * per):
        copies.append(
            pltpu.make_async_copy(x_hbm.at[j // per, pl.ds((j % per) * ROWS, ROWS), :], x_buf.at[pl.ds(j * ROWS, ROWS), :], x_sem.at[j])
        )
    for c in wcopies + scopies + copies:
        c.start()

    def dev(zz, t=None):
        return (grp, zz, tp if t is None else t)

    ends = []
    at = 0
    for size in sizes:
        at += size
        ends.append(at)
    starts = [e - size + 1 for e, size in zip(ends, sizes)]

    def among(values):
        hit = z == values[0]
        for v in values[1:]:
            hit = hit | (z == v)
        return hit

    def table(keys, values):
        out = jnp.int32(0)
        for k, v in zip(keys, values):
            out = jnp.where(z == k, jnp.int32(v), out)
        return out

    head = among(ends)
    first = among(starts)
    lc_recv = (z >= 1) & jnp.logical_not(first)
    lc_send = (z >= 1) & jnp.logical_not(head)
    pc_recv = head & (z > ends[0])
    pc_send = head & (z < last)
    prev_head = table(ends[1:], ends[:-1])
    next_head = table(ends[:-1], ends[1:])

    bar = pltpu.get_barrier_semaphore()

    @pl.when(z == 1)
    def _():
        for zz in range(2, n):
            pl.semaphore_signal(bar, inc=1, device_id=dev(zz), device_id_type=MESH)
        for k in range(1, ntp):
            pl.semaphore_signal(bar, inc=1, device_id=dev(z, lax.rem(tp + k, ntp)), device_id_type=MESH)
        for k in range(ntp):
            pl.semaphore_signal(bar, inc=1, device_id=dev(0, lax.rem(tp + k, ntp)), device_id_type=MESH)

    @pl.when(lc_send)
    def _():
        pl.semaphore_signal(bar, inc=1, device_id=dev(z + 1), device_id_type=MESH)

    @pl.when(pc_send)
    def _():
        pl.semaphore_signal(bar, inc=1, device_id=dev(next_head), device_id_type=MESH)

    @pl.when(z != last)
    def _():
        pl.semaphore_signal(bar, inc=1, device_id=dev(last), device_id_type=MESH)

    one = jnp.int32(1)
    zero = jnp.int32(0)
    expect = (
        jnp.where(z == 0, ntp, jnp.where(z == 1, ntp - 1, 1))
        + jnp.where(lc_recv, one, zero)
        + jnp.where(pc_recv, one, zero)
        + jnp.where(z == last, n - 1, 0)
    )
    scopies[8].wait()
    ow_out[...] = ow_ref[0].astype(F32)
    pl.semaphore_wait(bar, expect)

    @pl.when(lc_recv)
    def _():
        pl.semaphore_signal(rdy_lc, inc=1, device_id=dev(z - 1), device_id_type=MESH)

    @pl.when(pc_recv)
    def _():
        pl.semaphore_signal(rdy_pc, inc=1, device_id=dev(prev_head), device_id_type=MESH)

    @pl.when(z == last)
    def _():
        pl.semaphore_signal(rdy_b0, inc=1, device_id=dev(0), device_id_type=MESH)

    @pl.when(z == 0)
    def _():
        for k in range(ntp):
            pl.semaphore_signal(rdy_p0, inc=1, device_id=dev(1, lax.rem(tp + k, ntp)), device_id_type=MESH)

    def ow_copy():
        return pltpu.make_async_remote_copy(
            src_ref=ow_out, dst_ref=ow_all.at[z], send_sem=ow_ss, recv_sem=ow_rs.at[z], device_id=dev(1), device_id_type=MESH
        )

    @pl.when(z != 1)
    def _():
        ow_copy().start()

    @pl.when(z == 1)
    def _():
        ow_all[1] = ow_out[...]

    local_body(tp, prompts, seg, wcopies, copies, scopies[:8], bw_ref, dw_ref, shift_ref, rate_ref, extra_ref, ab_ref, w_buf, x_buf, kv_buf, m_buf, t_buf, y_buf)

    def lc_copy(src, c):
        return pltpu.make_async_remote_copy(
            src_ref=src.at[c], dst_ref=lc_in.at[c], send_sem=lc_ss.at[c], recv_sem=lc_rs.at[c], device_id=dev(z + 1), device_id_type=MESH
        )

    def pc_copy(src, c):
        return pltpu.make_async_remote_copy(
            src_ref=src.at[c], dst_ref=pc_in.at[c], send_sem=pc_ss.at[c], recv_sem=pc_rs.at[c], device_id=dev(next_head), device_id_type=MESH
        )

    def b0_copy(c):
        return pltpu.make_async_remote_copy(
            src_ref=ab_ref.at[HALF + c], dst_ref=b0_in.at[c], send_sem=b0_ss.at[c], recv_sem=b0_rs.at[c], device_id=dev(last), device_id_type=MESH
        )

    def set_rhs(dst, src):
        for p in range(prompts):
            a = jnp.concatenate([src[c, p] for c in range(HALF)], axis=0)
            dst[p] = right3(a)

    def lc_step(c, carry):
        lc_copy(ab_ref, c).wait_recv()
        for p in range(prompts):
            y = dot(left3(lc_in[c, p]), rhs[p])
            y = y + jnp.where(c >= HALF, ab_ref[c, p], 0.0)
            lc_out[c, p] = y
            comp[c, p] = y

        @pl.when(lc_send)
        def _():
            lc_copy(lc_out, c).start()

        return carry

    @pl.when(lc_send & first)
    def _():
        pl.semaphore_wait(rdy_lc, 1)
        for c in range(NCH):
            lc_copy(ab_ref, c).start()

    @pl.when((z == 1) & pc_send)
    def _():
        pl.semaphore_wait(rdy_pc, 1)
        for c in range(NCH):
            pc_copy(ab_ref, c).start()

    @pl.when(z == 0)
    def _():
        pl.semaphore_wait(rdy_b0, 1)
        for c in range(HALF):
            b0_copy(c).start()

    @pl.when(lc_recv)
    def _():
        set_rhs(rhs, ab_ref)

        @pl.when(lc_send)
        def _():
            pl.semaphore_wait(rdy_lc, 1)

        lax.fori_loop(0, HALF, lc_step, 0)

        @pl.when(lc_send)
        def _():
            lax.fori_loop(HALF, NCH, lc_step, 0)

    def pc_step(c, carry):
        pc_copy(ab_ref, c).wait_recv()
        for p in range(prompts):
            y = dot(left3(pc_in[c, p]), rhs2[p])
            pc_out[c, p] = y + jnp.where(c >= HALF, comp[c, p], 0.0)

        @pl.when(pc_send)
        def _():
            pc_copy(pc_out, c).start()

        return carry

    @pl.when(pc_recv)
    def _():
        @pl.when(first)
        def _():
            for c in range(NCH):
                comp[c] = ab_ref[c]

        set_rhs(rhs2, comp)

        @pl.when(pc_send)
        def _():
            pl.semaphore_wait(rdy_pc, 1)

        lax.fori_loop(0, HALF, pc_step, 0)

        @pl.when(lc_recv)
        def _():
            lax.fori_loop(HALF, NCH, lc_step, 0)

        @pl.when(z == last)
        def _():
            set_rhs(rhs, pc_out)
            for c in range(HALF):
                b0_copy(c).wait_recv()
            for p in range(prompts):
                start = jnp.concatenate([b0_in[c, p] for c in range(HALF)], axis=0)
                fin = dot(left3(start), rhs[p])
                for c in range(HALF):
                    comp[HALF + c, p] = comp[HALF + c, p] + fin[c * CH : (c + 1) * CH]

        lax.fori_loop(HALF, NCH, pc_step, 0)

    tile_per = CH // 8

    def st_copy(zz):
        t = zz // 2
        return pltpu.make_async_remote_copy(
            src_ref=pc_out.at[HALF + t // tile_per, :, pl.ds((t % tile_per) * 8, 8), :], dst_ref=st_in, send_sem=st_ss.at[zz], recv_sem=st_rs, device_id=dev(zz), device_id_type=MESH
        )

    def nm_copy():
        return pltpu.make_async_remote_copy(
            src_ref=nm_out, dst_ref=nm_in, send_sem=nm_ss, recv_sem=nm_rs, device_id=dev(1), device_id_type=MESH
        )

    order = []
    for k in range(n):
        for zz in (k, last - 1 - k):
            if zz not in order and 0 <= zz < last:
                order.append(zz)

    @pl.when(z == last)
    def _():
        query = q_ref[...].astype(F32)
        query = query * lax.rsqrt(jnp.sum(query * query, axis=-1, keepdims=True) + EPS) * DK**-0.5
        reads = []
        for p in range(prompts):
            fin = jnp.concatenate([pc_out[HALF + c, p] for c in range(HALF)], axis=0)
            qh, ql = split(jnp.broadcast_to(query[p : p + 1], (8, DK)))
            fh, fl = split(fin)
            read = lax.dot_general(
                jnp.concatenate([qh, ql, qh], axis=1), jnp.concatenate([fh, fh, fl], axis=1), NT, preferred_element_type=F32
            )
            reads.append(read[0:1])
        read = jnp.concatenate(reads, axis=0)
        scaled = read * lax.rsqrt(jnp.mean(read * read, axis=-1, keepdims=True) + EPS)
        gate = gate_ref[...].astype(F32)
        normed = (scaled * gain_ref[...] * (gate * jax.nn.sigmoid(gate))).astype(BF16)
        nm_out[...] = normed.astype(F32)
        nm_copy().start()
        for zz in order:
            st_copy(zz).start()
        t = last // 2
        for p in range(prompts):
            st_in[p] = pc_out[HALF + t // tile_per, p, (t % tile_per) * 8 : (t % tile_per) * 8 + 8, :]

    def pt_copy(k):
        return pltpu.make_async_remote_copy(
            src_ref=part.at[tp], dst_ref=part.at[tp], send_sem=pt_ss.at[k], recv_sem=pt_rs.at[k], device_id=dev(1, lax.rem(tp + k, ntp)), device_id_type=MESH
        )

    def p0_copy(k):
        return pltpu.make_async_remote_copy(
            src_ref=part.at[tp, 0], dst_ref=part0.at[k], send_sem=p0_ss.at[k], recv_sem=p0_rs.at[k], device_id=dev(0, lax.rem(tp + k, ntp)), device_id_type=MESH
        )

    def fin_copy(zz):
        return pltpu.make_async_remote_copy(
            src_ref=tot.at[zz // 2], dst_ref=fin_in, send_sem=fn_ss.at[zz], recv_sem=fn_rs, device_id=dev(zz), device_id_type=MESH
        )

    out_order = [zz for k in range(1, n) for zz in (1 + k, (1 - k) % n) if 1 < zz < n]
    out_order = [zz for i, zz in enumerate(out_order) if zz not in out_order[:i]]

    @pl.when(z == 1)
    def _():
        for zz in range(n):
            if zz != 1:
                pltpu.make_async_remote_copy(
                    src_ref=ow_out, dst_ref=ow_all.at[zz], send_sem=ow_ss, recv_sem=ow_rs.at[zz], device_id=dev(1), device_id_type=MESH
                ).wait_recv()
        lines = ow_all.shape[1]
        for r in range(lines):
            ow_mat[pl.ds(r * n, n), :] = ow_all[:, r, :].astype(BF16)
        vr = lax.broadcasted_iota(jnp.int32, (DK, DK), 0)
        vc = lax.broadcasted_iota(jnp.int32, (DK, DK), 1)
        perm = jnp.where(vc == (vr % lines) * n + vr // lines, 1.0, 0.0).astype(BF16)
        half = ow_mat.shape[1] // 4
        for h in range(4):
            ow_mat[:, pl.ds(h * half, half)] = dot(perm, ow_mat[:, pl.ds(h * half, half)]).astype(BF16)
        pl.semaphore_wait(rdy_p0, ntp)
        nm_copy().wait_recv()
        lhs = jnp.concatenate([nm_in[...], jnp.zeros((8 - prompts, DK), F32)], axis=0).astype(BF16)
        part[tp, 0] = dot(lhs, ow_mat[:, 0:128])[0:prompts]
        for k in range(ntp):
            p0_copy(k).start()
        res = dot(lhs, ow_mat[:, 128:])
        for t in range(1, tiles):
            part[tp, t] = res[0:prompts, (t - 1) * 128 : t * 128]
        for k in range(1, ntp):
            pt_copy(k).start()
        for k in range(1, ntp):
            pt_copy(k).wait_recv()
        acc = part[0]
        for k in range(1, ntp):
            acc = acc + part[k]
        tot[...] = acc
        for zz in out_order:
            fin_copy(zz).start()
        fin_in[...] = acc[0]

    @pl.when(z != last)
    def _():
        pltpu.make_async_remote_copy(
            src_ref=st_in, dst_ref=st_in, send_sem=st_ss.at[0], recv_sem=st_rs, device_id=dev(last), device_id_type=MESH
        ).wait_recv()

    odd = lax.rem(z, 2)
    for p in range(prompts):
        st_ref[p] = jnp.where(odd == 1, st_in[p, 4:8, :], st_in[p, 0:4, :]).astype(BF16)

    @pl.when(z > 1)
    def _():
        pltpu.make_async_remote_copy(
            src_ref=fin_in, dst_ref=fin_in, send_sem=fn_ss.at[0], recv_sem=fn_rs, device_id=dev(1), device_id_type=MESH
        ).wait_recv()

    @pl.when(z == 0)
    def _():
        for k in range(ntp):
            p0_copy(k).wait_recv()
        acc = part0[0]
        for k in range(1, ntp):
            acc = acc + part0[k]
        fin_in[...] = acc

    at = odd * (ntp * span) + tp * span
    value = fin_in[...]
    lane = lax.broadcasted_iota(jnp.int32, (128, span), 0)
    want = lax.broadcasted_iota(jnp.int32, (128, span), 1) + at
    v1, v2 = split(value)
    v3 = (value - v1.astype(F32) - v2.astype(F32)).astype(BF16)
    sel = jnp.where(lane == want, 1.0, 0.0).astype(BF16)
    ro_ref[...] = dot(jnp.concatenate([v1, v2, v3], axis=1), jnp.concatenate([sel, sel, sel], axis=0))

    @pl.when(z != 1)
    def _():
        ow_copy().wait_send()

    @pl.when(lc_send)
    def _():
        for c in range(NCH):
            lc_copy(lc_out, c).wait_send()

    @pl.when(pc_send)
    def _():
        for c in range(NCH):
            pc_copy(pc_out, c).wait_send()

    @pl.when(z == 0)
    def _():
        for c in range(HALF):
            b0_copy(c).wait_send()

    @pl.when(z == last)
    def _():
        for zz in range(n):
            if zz != last:
                st_copy(zz).wait_send()
        nm_copy().wait_send()

    @pl.when(z == 1)
    def _():
        for k in range(1, ntp):
            pt_copy(k).wait_send()
        for k in range(ntp):
            p0_copy(k).wait_send()
        for zz in range(2, n):
            fin_copy(zz).wait_send()


VM = pl.BlockSpec(memory_space=pltpu.VMEM)
ANY = pl.BlockSpec(memory_space=pl.ANY)


def fused(n, ntp, x, wk, wv, bw, shift, dw, rate, extra, q, gate, gain, ow):
    prompts, seg, width = x.shape
    total = prompts * seg
    groups = total // BLK
    chunks = total // ROWS
    lines = ow.shape[1]
    sizes = GROUPS if n == sum(GROUPS) + 1 else (1,) * (n - 1)
    span = ow.shape[2] // (n * ntp)
    tiles = ow.shape[2] // 128
    vm = pltpu.VMEM
    blk = vm((NCH, prompts, CH, DK), F32)
    dma = pltpu.SemaphoreType.DMA
    reg = pltpu.SemaphoreType.REGULAR
    square = vm((groups, BLK, BLK), F32)
    small = [vm(a.shape, a.dtype) for a in (bw, shift, dw, rate, extra, q, gate, gain, ow)]
    return pl.pallas_call(
        functools.partial(body, n, ntp, sizes),
        name="delta_states",
        out_shape=(
            jax.ShapeDtypeStruct((prompts, lines, DK), BF16),
            jax.ShapeDtypeStruct((prompts, span), F32),
        ),
        in_specs=[ANY] * 12,
        out_specs=(VM, VM),
        scratch_shapes=[
            vm((width, 2 * DK), BF16),
            vm((total, width), BF16),
            vm((total, 2 * DK), BF16),
            square, square, square,
            *small,
            blk, blk, blk, blk, blk, blk,
            vm((prompts, 3 * DK, DK), BF16),
            vm((prompts, 3 * DK, DK), BF16),
            vm((HALF, prompts, CH, DK), F32),
            vm((prompts, 8, DK), F32),
            vm((prompts, 8, DK), F32),
            vm((prompts, DK), F32),
            vm((prompts, DK), F32),
            vm((lines, ow.shape[2]), F32),
            vm((n, lines, ow.shape[2]), F32),
            vm((n * lines, ow.shape[2]), BF16),
            vm((ntp, tiles, prompts, 128), F32),
            vm((ntp, prompts, 128), F32),
            vm((tiles, prompts, 128), F32),
            vm((prompts, 128), F32),
            dma((chunks,)), dma((2,)), dma((9,)),
            dma((NCH,)), dma((NCH,)), dma((NCH,)), dma((NCH,)),
            dma((HALF,)), dma((HALF,)),
            dma((n,)), dma,
            dma, dma,
            dma, dma((n,)),
            dma((ntp,)), dma((ntp,)),
            dma((ntp,)), dma((ntp,)),
            dma((n,)), dma,
            reg, reg, reg, reg,
        ],
        compiler_params=pltpu.CompilerParams(collective_id=0, has_side_effects=True),
    )(x, wk, wv, bw, shift, dw, rate, extra, q, gate, gain, ow)


def hand_over(st_in, ro_in, st_out, ro_out, sem):
    copies = [pltpu.make_async_copy(st_in, st_out, sem.at[0]), pltpu.make_async_copy(ro_in, ro_out, sem.at[1])]
    for c in copies:
        c.start()
    for c in copies:
        c.wait()


def finish(st, ro):
    return pl.pallas_call(
        hand_over,
        name="hand_over",
        out_shape=(jax.ShapeDtypeStruct(st.shape, st.dtype), jax.ShapeDtypeStruct(ro.shape, ro.dtype)),
        in_specs=[ANY, ANY],
        out_specs=(ANY, ANY),
        scratch_shapes=[pltpu.SemaphoreType.DMA((2,))],
    )(st, ro)


def solution(mesh):
    n, ntp = mesh.shape["sp"], mesh.shape["tp"]

    def per_device(x, wk, wv, bw, shift, dw, rate, extra, q, gate, gain, ow):
        prompts, seg, width = x.shape
        st, ro = fused(n, ntp, x, wk, wv, bw.T, shift.reshape(1, -1), dw.T, rate.reshape(1, -1), extra.reshape(prompts, 1, seg), q, gate, gain.reshape(1, -1), ow)
        st, ro = finish(st, ro)
        return jnp.transpose(st, (0, 2, 1))[:, None], ro

    placed = (
        P("grp", "sp", None),
        P(None, "tp"),
        P(None, "tp"),
        P(),
        P(),
        P(),
        P(),
        P("grp", "sp", "tp"),
        P("grp", "tp"),
        P("grp", "tp"),
        P(),
        P("tp", "sp", None),
    )
    return jax.shard_map(
        per_device,
        mesh=mesh,
        in_specs=placed,
        out_specs=(P("grp", "tp", None, "sp"), P("grp", ("sp", "tp"))),
        check_vma=False,
    )
```

```python
import functools

import jax
import jax.numpy as jnp
from jax import lax
from jax.experimental import pallas as pl
from jax.experimental.pallas import tpu as pltpu
from jax.sharding import PartitionSpec as P

MESH = pl.DeviceIdType.MESH
EPS = 1e-06
F32 = jnp.float32
BF16 = jnp.bfloat16
DK = 128
BLK = 128
CH = 16
ROWS = 256
HALF = DK // CH
NCH = 2 * HALF
GROUPS = (1, 1, 1, 1, 1, 2, 2, 2, 2, 2, 3, 4, 4, 5)
NT = (((1,), (1,)), ((), ()))


def dot(a, b):
    return jnp.dot(a, b, preferred_element_type=F32)


def split(a):
    high = a.astype(BF16)
    return high, (a - high.astype(F32)).astype(BF16)


def left3(a):
    high, low = split(a)
    return jnp.concatenate([high, low, high], axis=1)


def right3(b):
    high, low = split(b)
    return jnp.concatenate([high, high, low], axis=0)


def left2(a):
    return jnp.concatenate(split(a), axis=1)


def dot3(a, b):
    return dot(left3(a), right3(b))


def local_body(middle, tp, prompts, seg, wcopies, copies, scopies, bw_ref, dw_ref, shift_ref, rate_ref, extra_ref, ab_ref, w_buf, x_buf, kv_buf, m_buf, t_buf, y_buf):
    rows = ROWS
    chunks = len(copies)
    for c in wcopies:
        c.wait()
    for c in copies[1:]:
        c.start()
    wbd = jnp.concatenate([bw_ref[...], dw_ref[...]], axis=0)
    raw = []
    for j in range(chunks):
        copies[j].wait()
        xs = x_buf[pl.ds(j * rows, rows), :]
        kv_buf[pl.ds(j * rows, rows), :] = dot(xs, w_buf[...]).astype(BF16)
        raw.append(lax.dot_general(wbd, xs, NT, preferred_element_type=F32))
    middle()
    for c in scopies:
        c.wait()
    groups = prompts * seg // BLK
    gp = seg // BLK
    heads = bw_ref.shape[0]
    head_lane = lax.broadcasted_iota(jnp.int32, (2 * heads, 1), 0)
    pick_b = head_lane == tp
    pick_d = head_lane == tp + heads

    def pack(pick):
        lines = []
        for g in range(groups):
            at = g * BLK
            block = raw[at // rows][:, at % rows : at % rows + BLK]
            lines.append(jnp.sum(jnp.where(pick, block, 0.0), axis=0, keepdims=True))
        return jnp.concatenate(lines, axis=0)

    beta_raw = pack(pick_b).astype(BF16).astype(F32)
    decay_raw = pack(pick_d).astype(BF16).astype(F32)
    extra = jnp.concatenate(
        [extra_ref[g // gp, :, pl.ds((g % gp) * BLK, BLK)] for g in range(groups)], axis=0
    )
    own = lax.broadcasted_iota(jnp.int32, (1, heads), 1) == tp
    shift = jnp.sum(jnp.where(own, shift_ref[...], 0.0), axis=1, keepdims=True)
    rate = jnp.sum(jnp.where(own, rate_ref[...], 0.0), axis=1, keepdims=True)
    beta = jax.nn.sigmoid(beta_raw + shift)
    softplus = jnp.maximum(decay_raw, 0.0) + jnp.log1p(jnp.exp(-jnp.abs(decay_raw)))
    log_decay = -rate * softplus + extra
    row = lax.broadcasted_iota(jnp.int32, (BLK, BLK), 0)
    col = lax.broadcasted_iota(jnp.int32, (BLK, BLK), 1)
    upto = jnp.where(row <= col, 1.0, 0.0).astype(BF16)
    l1 = log_decay.astype(BF16)
    l2 = (log_decay - l1.astype(F32)).astype(BF16)
    l3 = (log_decay - l1.astype(F32) - l2.astype(F32)).astype(BF16)
    cum = dot(jnp.concatenate([l1, l2, l3], axis=1), jnp.concatenate([upto, upto, upto], axis=0))
    cum_t = cum.T
    beta_t = beta.T
    eye = row == col
    upper = row < col
    ident = jnp.where(eye, 1.0, 0.0)
    neu = upper & ((row >> 3) == (col >> 3))
    norms = []
    for g in range(groups):
        k = kv_buf[pl.ds(g * BLK, BLK), pl.ds(0, DK)]
        gram = lax.dot_general(k, k, NT, preferred_element_type=F32)
        diag = jnp.where(eye, gram, 0.0)
        r_row = lax.rsqrt(jnp.sum(diag, axis=0, keepdims=True) + EPS)
        r_col = lax.rsqrt(jnp.sum(diag, axis=1, keepdims=True) + EPS)
        c_row = cum[g : g + 1, :]
        c_col = cum_t[:, g : g + 1]
        scale = jnp.exp(jnp.where(upper, c_row - c_col, 0.0)) * (beta[g : g + 1, :] * r_row) * r_col
        m = jnp.where(upper, gram * scale, 0.0)
        m_buf[g] = m
        t_buf[g] = jnp.where(neu, m, 0.0)
        norms.append((r_row, r_col))
    p2 = []
    for g in range(groups):
        p = t_buf[g]
        p2.append(dot3(p, p))
    for g in range(groups):
        p = t_buf[g]
        both = dot3(p2[g], jnp.concatenate([p2[g], p], axis=1))
        y_buf[g] = both[:, :BLK]
        t_buf[g] = ident - p + p2[g] - both[:, BLK:]
    for g in range(groups):
        q = t_buf[g]
        t_buf[g] = q + dot3(q, y_buf[g])
    s = 8
    while s < BLK:
        mask = ((row // (2 * s)) == (col // (2 * s))) & ((row // s) % 2 == 0) & ((col // s) % 2 == 1)
        for g in range(groups):
            y_buf[g] = dot3(jnp.where(mask, m_buf[g], 0.0), t_buf[g])
        for g in range(groups):
            t = t_buf[g]
            t_buf[g] = t - dot3(t, y_buf[g])
        s *= 2
    for g in range(groups):
        r_row, r_col = norms[g]
        c_row = cum[g : g + 1, :]
        last = cum[g : g + 1, BLK - 1 : BLK]
        t = t_buf[g] * (jnp.exp(last - c_row) * r_row)
        b_col = beta_t[:, g : g + 1]
        e_col = jnp.exp(cum_t[:, g : g + 1]) * r_col * b_col
        k = kv_buf[pl.ds(g * BLK, BLK), pl.ds(0, DK)]
        v = kv_buf[pl.ds(g * BLK, BLK), pl.ds(DK, DK)]
        k2 = jnp.concatenate([k, k], axis=0)
        f = dot(left2(jnp.concatenate([t * e_col, t * b_col], axis=0)), k2)
        kt = k.T
        vt = v.T
        a_part = dot(jnp.concatenate([kt, kt], axis=1), jnp.concatenate(split(f[:BLK]), axis=0))
        b_part = dot(jnp.concatenate([vt, vt], axis=1), jnp.concatenate(split(f[BLK:]), axis=0))
        y_buf2 = jnp.concatenate([ident * jnp.exp(last) - a_part, b_part], axis=0)
        if g % gp == 0:
            maps = []
        maps.append(y_buf2)
        if g % gp == gp - 1:
            while len(maps) > 1:
                nexts = []
                for a in range(0, len(maps), 2):
                    early, late = maps[a], maps[a + 1]
                    prod = dot3(early, late[:DK])
                    nexts.append(jnp.concatenate([prod[:DK], prod[DK:] + late[DK:]], axis=0))
                maps = nexts
            p = g // gp
            for c in range(NCH):
                ab_ref[c, p] = maps[0][c * CH : (c + 1) * CH]


def body(n, ntp, sizes, x_hbm, wk_hbm, wv_hbm, bw_hbm, shift_hbm, dw_hbm, rate_hbm, extra_hbm, q_hbm, gate_hbm, gain_hbm, ow_hbm, st_ref, ro_ref, w_buf, x_buf, kv_buf, m_buf, t_buf, y_buf, bw_ref, shift_ref, dw_ref, rate_ref, extra_ref, q_ref, gate_ref, gain_ref, ow_ref, ab_ref, lc_in, pc_in, lc_out, pc_out, comp, rhs, rhs2, b0_in, dummy, st_in, nm_out, nm_in, ow_out, ow_all, ow_mat, part, part0, tot, fin_in, st_size, fn_size, x_sem, w_sem, in_sem, lc_ss, lc_rs, pc_ss, pc_rs, b0_ss, b0_rs, st_ss, st_rs, nm_ss, nm_rs, ow_ss, ow_rs, pt_ss, pt_rs, p0_ss, p0_rs, fn_ss, fn_rs, rdy_lc, rdy_pc, rdy_b0, rdy_p0):
    grp = lax.axis_index("grp")
    z = lax.axis_index("sp")
    tp = lax.axis_index("tp")
    last = n - 1
    prompts, seg, width = x_hbm.shape
    tiles = tot.shape[0]
    span = ro_ref.shape[1]

    wcopies = [
        pltpu.make_async_copy(wk_hbm, w_buf.at[:, pl.ds(0, DK)], w_sem.at[0]),
        pltpu.make_async_copy(wv_hbm, w_buf.at[:, pl.ds(DK, DK)], w_sem.at[1]),
    ]
    wcopies += [pltpu.make_async_copy(bw_hbm, bw_ref, w_sem.at[2]), pltpu.make_async_copy(dw_hbm, dw_ref, w_sem.at[3])]
    small = [(shift_hbm, shift_ref), (rate_hbm, rate_ref), (extra_hbm, extra_ref), (q_hbm, q_ref), (gate_hbm, gate_ref), (gain_hbm, gain_ref), (ow_hbm, ow_ref)]
    scopies = [pltpu.make_async_copy(a, b, in_sem.at[i]) for i, (a, b) in enumerate(small)]
    per = seg // ROWS
    copies = []
    for j in range(prompts * per):
        copies.append(
            pltpu.make_async_copy(x_hbm.at[j // per, pl.ds((j % per) * ROWS, ROWS), :], x_buf.at[pl.ds(j * ROWS, ROWS), :], x_sem.at[j])
        )
    for c in wcopies:
        c.start()

    def dev(zz, t=None):
        return (grp, zz, tp if t is None else t)

    ends = []
    at = 0
    for size in sizes:
        at += size
        ends.append(at)
    starts = [e - size + 1 for e, size in zip(ends, sizes)]

    def among(values):
        hit = z == values[0]
        for v in values[1:]:
            hit = hit | (z == v)
        return hit

    def table(keys, values):
        out = jnp.int32(0)
        for k, v in zip(keys, values):
            out = jnp.where(z == k, jnp.int32(v), out)
        return out

    head = among(ends)
    first = among(starts)
    lc_recv = (z >= 1) & jnp.logical_not(first)
    lc_send = (z >= 1) & jnp.logical_not(head)
    pc_recv = head & (z > ends[0])
    pc_send = head & (z < last)
    prev_head = table(ends[1:], ends[:-1])
    next_head = table(ends[:-1], ends[1:])

    bar = pltpu.get_barrier_semaphore()

    @pl.when(z == 1)
    def _():
        for zz in range(2, n):
            pl.semaphore_signal(bar, inc=1, device_id=dev(zz), device_id_type=MESH)
        for k in range(1, ntp):
            pl.semaphore_signal(bar, inc=1, device_id=dev(z, lax.rem(tp + k, ntp)), device_id_type=MESH)
        for k in range(ntp):
            pl.semaphore_signal(bar, inc=1, device_id=dev(0, lax.rem(tp + k, ntp)), device_id_type=MESH)

    @pl.when(lc_send)
    def _():
        pl.semaphore_signal(bar, inc=1, device_id=dev(z + 1), device_id_type=MESH)

    @pl.when(pc_send)
    def _():
        pl.semaphore_signal(bar, inc=1, device_id=dev(next_head), device_id_type=MESH)

    @pl.when(z != last)
    def _():
        pl.semaphore_signal(bar, inc=1, device_id=dev(last), device_id_type=MESH)

    copies[0].start()
    for c in scopies:
        c.start()
    one = jnp.int32(1)
    zero = jnp.int32(0)
    expect = (
        jnp.where(z == 0, ntp, jnp.where(z == 1, ntp - 1, 1))
        + jnp.where(lc_recv, one, zero)
        + jnp.where(pc_recv, one, zero)
        + jnp.where(z == last, n - 1, 0)
    )
    def ow_copy():
        return pltpu.make_async_remote_copy(
            src_ref=ow_out, dst_ref=ow_all.at[z], send_sem=ow_ss, recv_sem=ow_rs, device_id=dev(1), device_id_type=MESH
        )

    def middle():
        scopies[6].wait()
        ow_out[...] = ow_ref[0].astype(F32)
        pl.semaphore_wait(bar, expect)

        @pl.when(lc_recv)
        def _():
            pl.semaphore_signal(rdy_lc, inc=1, device_id=dev(z - 1), device_id_type=MESH)

        @pl.when(pc_recv)
        def _():
            pl.semaphore_signal(rdy_pc, inc=1, device_id=dev(prev_head), device_id_type=MESH)

        @pl.when(z == last)
        def _():
            pl.semaphore_signal(rdy_b0, inc=1, device_id=dev(0), device_id_type=MESH)

        @pl.when(z == 0)
        def _():
            for k in range(ntp):
                pl.semaphore_signal(rdy_p0, inc=1, device_id=dev(1, lax.rem(tp + k, ntp)), device_id_type=MESH)

        @pl.when(z != 1)
        def _():
            ow_copy().start()

        @pl.when(z == 1)
        def _():
            ow_all[1] = ow_out[...]

    local_body(middle, tp, prompts, seg, wcopies, copies, scopies[:6], bw_ref, dw_ref, shift_ref, rate_ref, extra_ref, ab_ref, w_buf, x_buf, kv_buf, m_buf, t_buf, y_buf)

    def lc_copy(src, c):
        return pltpu.make_async_remote_copy(
            src_ref=src.at[c], dst_ref=lc_in.at[c], send_sem=lc_ss, recv_sem=lc_rs.at[c], device_id=dev(z + 1), device_id_type=MESH
        )

    def pc_copy(src, c):
        return pltpu.make_async_remote_copy(
            src_ref=src.at[c], dst_ref=pc_in.at[c], send_sem=pc_ss, recv_sem=pc_rs.at[c], device_id=dev(next_head), device_id_type=MESH
        )

    def b0_copy():
        return pltpu.make_async_remote_copy(
            src_ref=ab_ref.at[pl.ds(HALF, HALF)], dst_ref=b0_in, send_sem=b0_ss, recv_sem=b0_rs, device_id=dev(last), device_id_type=MESH
        )

    def set_rhs(dst, src):
        for p in range(prompts):
            a = jnp.concatenate([src[c, p] for c in range(HALF)], axis=0)
            dst[p] = right3(a)

    def lc_step(c, carry):
        lc_copy(ab_ref, c).wait_recv()
        for p in range(prompts):
            y = dot(left3(lc_in[c, p]), rhs[p])
            y = y + jnp.where(c >= HALF, ab_ref[c, p], 0.0)
            lc_out[c, p] = y
            comp[c, p] = y

        @pl.when(lc_send)
        def _():
            lc_copy(lc_out, c).start()

        return carry

    @pl.when(lc_send & first)
    def _():
        pl.semaphore_wait(rdy_lc, 1)
        for c in range(NCH):
            lc_copy(ab_ref, c).start()

    @pl.when((z == 1) & pc_send)
    def _():
        pl.semaphore_wait(rdy_pc, 1)
        for c in range(NCH):
            pc_copy(ab_ref, c).start()

    @pl.when(z == 0)
    def _():
        pl.semaphore_wait(rdy_b0, 1)
        b0_copy().start()

    @pl.when(lc_recv)
    def _():
        set_rhs(rhs, ab_ref)

        @pl.when(lc_send)
        def _():
            pl.semaphore_wait(rdy_lc, 1)

        lax.fori_loop(0, HALF, lc_step, 0)

        @pl.when(lc_send | (z == last))
        def _():
            lax.fori_loop(HALF, NCH, lc_step, 0)

    def pc_step(c, carry):
        pc_copy(ab_ref, c).wait_recv()
        for p in range(prompts):
            y = dot(left3(pc_in[c, p]), rhs2[p])
            pc_out[c, p] = y + jnp.where(c >= HALF, comp[c, p], 0.0)

        @pl.when(pc_send)
        def _():
            pc_copy(pc_out, c).start()

        return carry

    @pl.when(pc_recv)
    def _():
        @pl.when(first)
        def _():
            for c in range(NCH):
                comp[c] = ab_ref[c]

        set_rhs(rhs2, comp)

        @pl.when(pc_send)
        def _():
            pl.semaphore_wait(rdy_pc, 1)

        lax.fori_loop(0, HALF, pc_step, 0)

        @pl.when(lc_recv & (z != last))
        def _():
            lax.fori_loop(HALF, NCH, lc_step, 0)

        @pl.when(z == last)
        def _():
            set_rhs(rhs, pc_out)
            b0_copy().wait_recv()
            for p in range(prompts):
                start = jnp.concatenate([b0_in[c, p] for c in range(HALF)], axis=0)
                fin = dot(left3(start), rhs[p])
                for c in range(HALF):
                    comp[HALF + c, p] = comp[HALF + c, p] + fin[c * CH : (c + 1) * CH]

        lax.fori_loop(HALF, NCH, pc_step, 0)

    tile_per = CH // 8

    def st_copy(zz):
        t = zz // 2
        return pltpu.make_async_remote_copy(
            src_ref=pc_out.at[HALF + t // tile_per, :, pl.ds((t % tile_per) * 8, 8), :], dst_ref=st_in, send_sem=st_ss, recv_sem=st_rs, device_id=dev(zz), device_id_type=MESH
        )

    def nm_copy():
        return pltpu.make_async_remote_copy(
            src_ref=nm_out, dst_ref=nm_in, send_sem=nm_ss, recv_sem=nm_rs, device_id=dev(1), device_id_type=MESH
        )

    order = []
    for k in range(n):
        for zz in (k, last - 1 - k):
            if zz not in order and 0 <= zz < last:
                order.append(zz)

    @pl.when(z == last)
    def _():
        query = q_ref[...].astype(F32)
        query = query * lax.rsqrt(jnp.sum(query * query, axis=-1, keepdims=True) + EPS) * DK**-0.5
        reads = []
        for p in range(prompts):
            fin = jnp.concatenate([pc_out[HALF + c, p] for c in range(HALF)], axis=0)
            qh, ql = split(jnp.broadcast_to(query[p : p + 1], (8, DK)))
            fh, fl = split(fin)
            read = lax.dot_general(
                jnp.concatenate([qh, ql, qh], axis=1), jnp.concatenate([fh, fh, fl], axis=1), NT, preferred_element_type=F32
            )
            reads.append(read[0:1])
        read = jnp.concatenate(reads, axis=0)
        scaled = read * lax.rsqrt(jnp.mean(read * read, axis=-1, keepdims=True) + EPS)
        gate = gate_ref[...].astype(F32)
        normed = (scaled * gain_ref[...] * (gate * jax.nn.sigmoid(gate))).astype(BF16)
        nm_out[...] = normed.astype(F32)
        nm_copy().start()
        for zz in order:
            st_copy(zz).start()
        t = last // 2
        for p in range(prompts):
            st_in[p] = pc_out[HALF + t // tile_per, p, (t % tile_per) * 8 : (t % tile_per) * 8 + 8, :]

    def pt_copy(k):
        return pltpu.make_async_remote_copy(
            src_ref=part.at[tp], dst_ref=part.at[tp], send_sem=pt_ss, recv_sem=pt_rs, device_id=dev(1, lax.rem(tp + k, ntp)), device_id_type=MESH
        )

    def pt_all():
        some = part.at[pl.ds(0, ntp - 1)]
        return pltpu.make_async_remote_copy(
            src_ref=some, dst_ref=some, send_sem=pt_ss, recv_sem=pt_rs, device_id=dev(0), device_id_type=MESH
        )

    def p0_all():
        return pltpu.make_async_remote_copy(
            src_ref=part0, dst_ref=part0, send_sem=p0_ss, recv_sem=p0_rs, device_id=dev(last), device_id_type=MESH
        )

    def p0_copy(k):
        return pltpu.make_async_remote_copy(
            src_ref=part.at[tp, 0], dst_ref=part0.at[tp], send_sem=p0_ss, recv_sem=p0_rs, device_id=dev(0, lax.rem(tp + k, ntp)), device_id_type=MESH
        )

    def fin_copy(zz):
        return pltpu.make_async_remote_copy(
            src_ref=tot.at[zz // 2], dst_ref=fin_in, send_sem=fn_ss, recv_sem=fn_rs, device_id=dev(zz), device_id_type=MESH
        )

    out_order = [zz for k in range(1, n) for zz in (1 + k, (1 - k) % n) if 1 < zz < n]
    out_order = [zz for i, zz in enumerate(out_order) if zz not in out_order[:i]]

    @pl.when(z == 1)
    def _():
        pltpu.make_async_remote_copy(
            src_ref=ow_all.at[pl.ds(0, n - 1)], dst_ref=ow_all.at[pl.ds(0, n - 1)], send_sem=ow_ss, recv_sem=ow_rs, device_id=dev(0), device_id_type=MESH
        ).wait_recv()
        lines = ow_all.shape[1]
        for r in range(lines):
            ow_mat[pl.ds(r * n, n), :] = ow_all[:, r, :].astype(BF16)
        vr = lax.broadcasted_iota(jnp.int32, (DK, DK), 0)
        vc = lax.broadcasted_iota(jnp.int32, (DK, DK), 1)
        perm = jnp.where(vc == (vr % lines) * n + vr // lines, 1.0, 0.0).astype(BF16)
        half = ow_mat.shape[1] // 4
        for h in range(4):
            ow_mat[:, pl.ds(h * half, half)] = dot(perm, ow_mat[:, pl.ds(h * half, half)]).astype(BF16)
        pl.semaphore_wait(rdy_p0, ntp)
        nm_copy().wait_recv()
        lhs = jnp.concatenate([nm_in[...], jnp.zeros((8 - prompts, DK), F32)], axis=0).astype(BF16)
        part[tp, 0] = dot(lhs, ow_mat[:, 0:128])[0:prompts]
        for k in range(ntp):
            p0_copy(k).start()
        res = dot(lhs, ow_mat[:, 128:])
        for t in range(1, tiles):
            part[tp, t] = res[0:prompts, (t - 1) * 128 : t * 128]
        for k in range(1, ntp):
            pt_copy(k).start()
        pt_all().wait_recv()
        acc = part[0]
        for k in range(1, ntp):
            acc = acc + part[k]
        tot[...] = acc
        for zz in out_order:
            fin_copy(zz).start()
        fin_in[...] = acc[0]

    @pl.when(z != last)
    def _():
        pltpu.make_async_remote_copy(
            src_ref=st_in, dst_ref=st_in, send_sem=st_ss, recv_sem=st_rs, device_id=dev(last), device_id_type=MESH
        ).wait_recv()

    odd = lax.rem(z, 2)
    for p in range(prompts):
        st_ref[p] = jnp.where(odd == 1, st_in[p, 4:8, :], st_in[p, 0:4, :]).astype(BF16)

    @pl.when(z > 1)
    def _():
        pltpu.make_async_remote_copy(
            src_ref=fin_in, dst_ref=fin_in, send_sem=fn_ss, recv_sem=fn_rs, device_id=dev(1), device_id_type=MESH
        ).wait_recv()

    @pl.when(z == 0)
    def _():
        p0_all().wait_recv()
        acc = part0[0]
        for k in range(1, ntp):
            acc = acc + part0[k]
        fin_in[...] = acc

    at = odd * (ntp * span) + tp * span
    value = fin_in[...]
    lane = lax.broadcasted_iota(jnp.int32, (128, span), 0)
    want = lax.broadcasted_iota(jnp.int32, (128, span), 1) + at
    v1, v2 = split(value)
    v3 = (value - v1.astype(F32) - v2.astype(F32)).astype(BF16)
    sel = jnp.where(lane == want, 1.0, 0.0).astype(BF16)
    ro_ref[...] = dot(jnp.concatenate([v1, v2, v3], axis=1), jnp.concatenate([sel, sel, sel], axis=0))

    @pl.when(z != 1)
    def _():
        ow_copy().wait_send()

    @pl.when(lc_send)
    def _():
        pltpu.make_async_remote_copy(
            src_ref=lc_out, dst_ref=lc_in, send_sem=lc_ss, recv_sem=lc_rs.at[0], device_id=dev(z + 1), device_id_type=MESH
        ).wait_send()

    @pl.when(pc_send)
    def _():
        pltpu.make_async_remote_copy(
            src_ref=pc_out, dst_ref=pc_in, send_sem=pc_ss, recv_sem=pc_rs.at[0], device_id=dev(next_head), device_id_type=MESH
        ).wait_send()

    @pl.when(z == 0)
    def _():
        b0_copy().wait_send()

    @pl.when(z == last)
    def _():
        pltpu.make_async_remote_copy(
            src_ref=st_size, dst_ref=st_size, send_sem=st_ss, recv_sem=st_rs, device_id=dev(0), device_id_type=MESH
        ).wait_send()
        nm_copy().wait_send()

    @pl.when(z == 1)
    def _():
        pt_all().wait_send()
        p0_all().wait_send()
        pltpu.make_async_remote_copy(
            src_ref=fn_size, dst_ref=fn_size, send_sem=fn_ss, recv_sem=fn_rs, device_id=dev(0), device_id_type=MESH
        ).wait_send()


VM = pl.BlockSpec(memory_space=pltpu.VMEM)
ANY = pl.BlockSpec(memory_space=pl.ANY)


def fused(n, ntp, x, wk, wv, bw, shift, dw, rate, extra, q, gate, gain, ow):
    prompts, seg, width = x.shape
    total = prompts * seg
    groups = total // BLK
    chunks = total // ROWS
    lines = ow.shape[1]
    sizes = GROUPS if n == sum(GROUPS) + 1 else (1,) * (n - 1)
    span = ow.shape[2] // (n * ntp)
    tiles = ow.shape[2] // 128
    vm = pltpu.VMEM
    blk = vm((NCH, prompts, CH, DK), F32)
    dma = pltpu.SemaphoreType.DMA
    reg = pltpu.SemaphoreType.REGULAR
    square = vm((groups, BLK, BLK), F32)
    small = [vm(a.shape, a.dtype) for a in (bw, shift, dw, rate, extra, q, gate, gain, ow)]
    return pl.pallas_call(
        functools.partial(body, n, ntp, sizes),
        name="delta_states",
        out_shape=(
            pltpu.VMEM((prompts, lines, DK), BF16),
            pltpu.VMEM((prompts, span), F32),
        ),
        in_specs=[ANY] * 12,
        out_specs=(VM, VM),
        scratch_shapes=[
            vm((width, 2 * DK), BF16),
            vm((total, width), BF16),
            vm((total, 2 * DK), BF16),
            square, square, square,
            *small,
            blk, blk, blk, blk, blk, blk,
            vm((prompts, 3 * DK, DK), BF16),
            vm((prompts, 3 * DK, DK), BF16),
            vm((HALF, prompts, CH, DK), F32),
            vm((prompts, 8, DK), F32),
            vm((prompts, 8, DK), F32),
            vm((prompts, DK), F32),
            vm((prompts, DK), F32),
            vm((lines, ow.shape[2]), F32),
            vm((n, lines, ow.shape[2]), F32),
            vm((n * lines, ow.shape[2]), BF16),
            vm((ntp, tiles, prompts, 128), F32),
            vm((ntp, prompts, 128), F32),
            vm((tiles, prompts, 128), F32),
            vm((prompts, 128), F32),
            vm((n - 1, prompts, 8, DK), F32),
            vm((n - 2, prompts, 128), F32),
            dma((chunks,)), dma((4,)), dma((7,)),
            dma, dma((NCH,)), dma, dma((NCH,)),
            dma, dma,
            dma, dma,
            dma, dma,
            dma, dma,
            dma, dma,
            dma, dma,
            dma, dma,
            reg, reg, reg, reg,
        ],
        compiler_params=pltpu.CompilerParams(collective_id=0, has_side_effects=True),
    )(x, wk, wv, bw, shift, dw, rate, extra, q, gate, gain, ow)


def hand_over(st_in, ro_in, st_out, ro_out, sem):
    copies = [pltpu.make_async_copy(st_in, st_out, sem.at[0]), pltpu.make_async_copy(ro_in, ro_out, sem.at[1])]
    for c in copies:
        c.start()
    for c in copies:
        c.wait()


def finish(st, ro):
    return pl.pallas_call(
        hand_over,
        name="hand_over",
        out_shape=(jax.ShapeDtypeStruct(st.shape, st.dtype), jax.ShapeDtypeStruct(ro.shape, ro.dtype)),
        in_specs=[ANY, ANY],
        out_specs=(ANY, ANY),
        scratch_shapes=[pltpu.SemaphoreType.DMA((2,))],
        compiler_params=pltpu.CompilerParams(vmem_limit_bytes=1024 * 1024),
    )(st, ro)


def solution(mesh):
    n, ntp = mesh.shape["sp"], mesh.shape["tp"]

    def per_device(x, wk, wv, bw, shift, dw, rate, extra, q, gate, gain, ow):
        prompts, seg, width = x.shape
        st, ro = fused(n, ntp, x, wk, wv, bw.T, shift.reshape(1, -1), dw.T, rate.reshape(1, -1), extra.reshape(prompts, 1, seg), q, gate, gain.reshape(1, -1), ow)
        st, ro = finish(st, ro)
        return jnp.transpose(st, (0, 2, 1))[:, None], ro

    placed = (
        P("grp", "sp", None),
        P(None, "tp"),
        P(None, "tp"),
        P(),
        P(),
        P(),
        P(),
        P("grp", "sp", "tp"),
        P("grp", "tp"),
        P("grp", "tp"),
        P(),
        P("tp", "sp", None),
    )
    return jax.shard_map(
        per_device,
        mesh=mesh,
        in_specs=placed,
        out_specs=(P("grp", "tp", None, "sp"), P("grp", ("sp", "tp"))),
        check_vma=False,
    )
```

```python
import functools

import jax
import jax.numpy as jnp
from jax import lax
from jax.experimental import pallas as pl
from jax.experimental.pallas import tpu as pltpu
from jax.sharding import PartitionSpec as P

MESH = pl.DeviceIdType.MESH
EPS = 1e-06
F32 = jnp.float32
BF16 = jnp.bfloat16
DK = 128
BLK = 128
CH = 16
ROWS = 256
HALF = DK // CH
NCH = 2 * HALF
GROUPS = (1, 1, 1, 1, 1, 2, 2, 2, 2, 2, 3, 4, 4, 5)
NT = (((1,), (1,)), ((), ()))


def dot(a, b):
    return jnp.dot(a, b, preferred_element_type=F32)


def split(a):
    high = a.astype(BF16)
    return high, (a - high.astype(F32)).astype(BF16)


def left3(a):
    high, low = split(a)
    return jnp.concatenate([high, low, high], axis=1)


def right3(b):
    high, low = split(b)
    return jnp.concatenate([high, high, low], axis=0)


def left2(a):
    return jnp.concatenate(split(a), axis=1)


def dot3(a, b):
    return dot(left3(a), right3(b))


def local_body(middle, tp, prompts, seg, wcopies, copies, scopies, bw_ref, dw_ref, shift_ref, rate_ref, extra_ref, ab_ref, w_buf, x_buf, kv_buf, m_buf, t_buf, y_buf):
    rows = ROWS
    chunks = len(copies)
    for c in wcopies:
        c.wait()
    for c in copies[1:]:
        c.start()
    wbd = jnp.concatenate([bw_ref[...], dw_ref[...]], axis=0)
    raw = []
    for j in range(chunks):
        copies[j].wait()
        xs = x_buf[pl.ds(j * rows, rows), :]
        kv_buf[pl.ds(j * rows, rows), :] = dot(xs, w_buf[...]).astype(BF16)
        raw.append(lax.dot_general(wbd, xs, NT, preferred_element_type=F32))
    middle()
    for c in scopies:
        c.wait()
    groups = prompts * seg // BLK
    gp = seg // BLK
    heads = bw_ref.shape[0]
    head_lane = lax.broadcasted_iota(jnp.int32, (2 * heads, 1), 0)
    pick_b = head_lane == tp
    pick_d = head_lane == tp + heads

    def pack(pick):
        lines = []
        for g in range(groups):
            at = g * BLK
            block = raw[at // rows][:, at % rows : at % rows + BLK]
            lines.append(jnp.sum(jnp.where(pick, block, 0.0), axis=0, keepdims=True))
        return jnp.concatenate(lines, axis=0)

    beta_raw = pack(pick_b).astype(BF16).astype(F32)
    decay_raw = pack(pick_d).astype(BF16).astype(F32)
    extra = jnp.concatenate(
        [extra_ref[g // gp, :, pl.ds((g % gp) * BLK, BLK)] for g in range(groups)], axis=0
    )
    own = lax.broadcasted_iota(jnp.int32, (1, heads), 1) == tp
    shift = jnp.sum(jnp.where(own, shift_ref[...], 0.0), axis=1, keepdims=True)
    rate = jnp.sum(jnp.where(own, rate_ref[...], 0.0), axis=1, keepdims=True)
    beta = jax.nn.sigmoid(beta_raw + shift)
    softplus = jnp.maximum(decay_raw, 0.0) + jnp.log1p(jnp.exp(-jnp.abs(decay_raw)))
    log_decay = -rate * softplus + extra
    row = lax.broadcasted_iota(jnp.int32, (BLK, BLK), 0)
    col = lax.broadcasted_iota(jnp.int32, (BLK, BLK), 1)
    upto = jnp.where(row <= col, 1.0, 0.0).astype(BF16)
    l1 = log_decay.astype(BF16)
    l2 = (log_decay - l1.astype(F32)).astype(BF16)
    l3 = (log_decay - l1.astype(F32) - l2.astype(F32)).astype(BF16)
    cum = dot(jnp.concatenate([l1, l2, l3], axis=1), jnp.concatenate([upto, upto, upto], axis=0))
    cum_t = cum.T
    beta_t = beta.T
    eye = row == col
    upper = row < col
    ident = jnp.where(eye, 1.0, 0.0)
    neu = upper & ((row >> 3) == (col >> 3))
    norms = []
    for g in range(groups):
        k = kv_buf[pl.ds(g * BLK, BLK), pl.ds(0, DK)]
        gram = lax.dot_general(k, k, NT, preferred_element_type=F32)
        diag = jnp.where(eye, gram, 0.0)
        r_row = lax.rsqrt(jnp.sum(diag, axis=0, keepdims=True) + EPS)
        r_col = lax.rsqrt(jnp.sum(diag, axis=1, keepdims=True) + EPS)
        c_row = cum[g : g + 1, :]
        c_col = cum_t[:, g : g + 1]
        scale = jnp.exp(jnp.where(upper, c_row - c_col, 0.0)) * (beta[g : g + 1, :] * r_row) * r_col
        m = jnp.where(upper, gram * scale, 0.0)
        m_buf[g] = m
        t_buf[g] = jnp.where(neu, m, 0.0)
        norms.append((r_row, r_col))
    p2 = []
    for g in range(groups):
        p = t_buf[g]
        p2.append(dot3(p, p))
    for g in range(groups):
        p = t_buf[g]
        both = dot3(p2[g], jnp.concatenate([p2[g], p], axis=1))
        y_buf[g] = both[:, :BLK]
        t_buf[g] = ident - p + p2[g] - both[:, BLK:]
    for g in range(groups):
        q = t_buf[g]
        t_buf[g] = q + dot3(q, y_buf[g])
    s = 8
    while s < BLK:
        mask = ((row // (2 * s)) == (col // (2 * s))) & ((row // s) % 2 == 0) & ((col // s) % 2 == 1)
        for g in range(groups):
            y_buf[g] = dot3(jnp.where(mask, m_buf[g], 0.0), t_buf[g])
        for g in range(groups):
            t = t_buf[g]
            t_buf[g] = t - dot3(t, y_buf[g])
        s *= 2
    for g in range(groups):
        r_row, r_col = norms[g]
        c_row = cum[g : g + 1, :]
        last = cum[g : g + 1, BLK - 1 : BLK]
        t = t_buf[g] * (jnp.exp(last - c_row) * r_row)
        b_col = beta_t[:, g : g + 1]
        e_col = jnp.exp(cum_t[:, g : g + 1]) * r_col * b_col
        k = kv_buf[pl.ds(g * BLK, BLK), pl.ds(0, DK)]
        v = kv_buf[pl.ds(g * BLK, BLK), pl.ds(DK, DK)]
        k2 = jnp.concatenate([k, k], axis=0)
        f = dot(left2(jnp.concatenate([t * e_col, t * b_col], axis=0)), k2)
        kt = k.T
        vt = v.T
        a_part = dot(jnp.concatenate([kt, kt], axis=1), jnp.concatenate(split(f[:BLK]), axis=0))
        b_part = dot(jnp.concatenate([vt, vt], axis=1), jnp.concatenate(split(f[BLK:]), axis=0))
        y_buf2 = jnp.concatenate([ident * jnp.exp(last) - a_part, b_part], axis=0)
        if g % gp == 0:
            maps = []
        maps.append(y_buf2)
        if g % gp == gp - 1:
            while len(maps) > 1:
                nexts = []
                for a in range(0, len(maps), 2):
                    early, late = maps[a], maps[a + 1]
                    prod = dot3(early, late[:DK])
                    nexts.append(jnp.concatenate([prod[:DK], prod[DK:] + late[DK:]], axis=0))
                maps = nexts
            p = g // gp
            for c in range(NCH):
                ab_ref[c, p] = maps[0][c * CH : (c + 1) * CH]


def body(n, ntp, sizes, x_hbm, wk_hbm, wv_hbm, bw_hbm, shift_hbm, dw_hbm, rate_hbm, extra_hbm, q_hbm, gate_hbm, gain_hbm, ow_hbm, st_ref, ro_ref, w_buf, x_buf, kv_buf, m_buf, t_buf, y_buf, bw_ref, shift_ref, dw_ref, rate_ref, extra_ref, q_ref, gate_ref, gain_ref, ow_ref, ab_ref, lc_in, pc_in, lc_out, pc_out, comp, rhs, rhs2, b0_in, dummy, st_in, nm_out, nm_in, ow_out, ow_all, ow_mat, part, part0, tot, fin_in, st_size, fn_size, x_sem, w_sem, in_sem, lc_ss, lc_rs, pc_ss, pc_rs, b0_ss, b0_rs, st_ss, st_rs, nm_ss, nm_rs, ow_ss, ow_rs, pt_ss, pt_rs, p0_ss, p0_rs, fn_ss, fn_rs, rdy_lc, rdy_pc, rdy_b0, rdy_p0):
    grp = lax.axis_index("grp")
    z = lax.axis_index("sp")
    tp = lax.axis_index("tp")
    last = n - 1
    prompts, seg, width = x_hbm.shape
    tiles = tot.shape[0]
    span = ro_ref.shape[1]

    wcopies = [
        pltpu.make_async_copy(wk_hbm, w_buf.at[:, pl.ds(0, DK)], w_sem.at[0]),
        pltpu.make_async_copy(wv_hbm, w_buf.at[:, pl.ds(DK, DK)], w_sem.at[1]),
    ]
    wcopies += [pltpu.make_async_copy(bw_hbm, bw_ref, w_sem.at[2]), pltpu.make_async_copy(dw_hbm, dw_ref, w_sem.at[3])]
    small = [(shift_hbm, shift_ref), (rate_hbm, rate_ref), (extra_hbm, extra_ref), (q_hbm, q_ref), (gate_hbm, gate_ref), (gain_hbm, gain_ref), (ow_hbm, ow_ref)]
    scopies = [pltpu.make_async_copy(a, b, in_sem.at[i]) for i, (a, b) in enumerate(small)]
    per = seg // ROWS
    copies = []
    for j in range(prompts * per):
        copies.append(
            pltpu.make_async_copy(x_hbm.at[j // per, pl.ds((j % per) * ROWS, ROWS), :], x_buf.at[pl.ds(j * ROWS, ROWS), :], x_sem.at[j])
        )
    for c in wcopies:
        c.start()

    def dev(zz, t=None):
        return (grp, zz, tp if t is None else t)

    ends = []
    at = 0
    for size in sizes:
        at += size
        ends.append(at)
    starts = [e - size + 1 for e, size in zip(ends, sizes)]

    def among(values):
        hit = z == values[0]
        for v in values[1:]:
            hit = hit | (z == v)
        return hit

    def table(keys, values):
        out = jnp.int32(0)
        for k, v in zip(keys, values):
            out = jnp.where(z == k, jnp.int32(v), out)
        return out

    head = among(ends)
    first = among(starts)
    lc_recv = (z >= 1) & jnp.logical_not(first)
    lc_send = (z >= 1) & jnp.logical_not(head)
    carry = tp == 0
    late = (z == 0) & carry
    opens = (z == 0) & jnp.logical_not(carry)
    pc_recv = head & ((z > ends[0]) | jnp.logical_not(carry))
    pc_send = (head & (z < last)) | opens
    prev_head = table(ends[1:], ends[:-1])
    next_head = jnp.where(z == 0, ends[0], table(ends[:-1], ends[1:]))

    bar = pltpu.get_barrier_semaphore()

    @pl.when(z == 1)
    def _():
        for zz in range(2, n):
            pl.semaphore_signal(bar, inc=1, device_id=dev(zz), device_id_type=MESH)
        for k in range(1, ntp):
            pl.semaphore_signal(bar, inc=1, device_id=dev(z, lax.rem(tp + k, ntp)), device_id_type=MESH)
        for k in range(ntp):
            pl.semaphore_signal(bar, inc=1, device_id=dev(0, lax.rem(tp + k, ntp)), device_id_type=MESH)

    @pl.when(lc_send)
    def _():
        pl.semaphore_signal(bar, inc=1, device_id=dev(z + 1), device_id_type=MESH)

    @pl.when(pc_send)
    def _():
        pl.semaphore_signal(bar, inc=1, device_id=dev(next_head), device_id_type=MESH)

    @pl.when(z != last)
    def _():
        pl.semaphore_signal(bar, inc=1, device_id=dev(last), device_id_type=MESH)

    copies[0].start()
    for c in scopies:
        c.start()
    one = jnp.int32(1)
    zero = jnp.int32(0)
    expect = (
        jnp.where(z == 0, ntp, jnp.where(z == 1, ntp - 1, 1))
        + jnp.where(lc_recv, one, zero)
        + jnp.where(pc_recv, one, zero)
        + jnp.where(z == last, n - 1, 0)
    )
    def ow_copy():
        return pltpu.make_async_remote_copy(
            src_ref=ow_out, dst_ref=ow_all.at[z], send_sem=ow_ss, recv_sem=ow_rs, device_id=dev(1), device_id_type=MESH
        )

    def middle():
        scopies[6].wait()
        ow_out[...] = ow_ref[0].astype(F32)
        pl.semaphore_wait(bar, expect)

        @pl.when(lc_recv)
        def _():
            pl.semaphore_signal(rdy_lc, inc=1, device_id=dev(z - 1), device_id_type=MESH)

        @pl.when(pc_recv)
        def _():
            pl.semaphore_signal(rdy_pc, inc=1, device_id=dev(prev_head), device_id_type=MESH)

        @pl.when((z == last) & carry)
        def _():
            pl.semaphore_signal(rdy_b0, inc=1, device_id=dev(0), device_id_type=MESH)

        @pl.when(z == 0)
        def _():
            for k in range(ntp):
                pl.semaphore_signal(rdy_p0, inc=1, device_id=dev(1, lax.rem(tp + k, ntp)), device_id_type=MESH)

        @pl.when(z != 1)
        def _():
            ow_copy().start()

        @pl.when(z == 1)
        def _():
            ow_all[1] = ow_out[...]

    local_body(middle, tp, prompts, seg, wcopies, copies, scopies[:6], bw_ref, dw_ref, shift_ref, rate_ref, extra_ref, ab_ref, w_buf, x_buf, kv_buf, m_buf, t_buf, y_buf)

    def lc_copy(src, c):
        return pltpu.make_async_remote_copy(
            src_ref=src.at[c], dst_ref=lc_in.at[c], send_sem=lc_ss, recv_sem=lc_rs.at[c], device_id=dev(z + 1), device_id_type=MESH
        )

    def pc_copy(src, c):
        return pltpu.make_async_remote_copy(
            src_ref=src.at[c], dst_ref=pc_in.at[c], send_sem=pc_ss, recv_sem=pc_rs.at[c], device_id=dev(next_head), device_id_type=MESH
        )

    def b0_copy():
        return pltpu.make_async_remote_copy(
            src_ref=ab_ref.at[pl.ds(HALF, HALF)], dst_ref=b0_in, send_sem=b0_ss, recv_sem=b0_rs, device_id=dev(last), device_id_type=MESH
        )

    def set_rhs(dst, src):
        for p in range(prompts):
            a = jnp.concatenate([src[c, p] for c in range(HALF)], axis=0)
            dst[p] = right3(a)

    def lc_step(c, carry):
        lc_copy(ab_ref, c).wait_recv()
        for p in range(prompts):
            y = dot(left3(lc_in[c, p]), rhs[p])
            y = y + jnp.where(c >= HALF, ab_ref[c, p], 0.0)
            lc_out[c, p] = y
            comp[c, p] = y

        @pl.when(lc_send)
        def _():
            lc_copy(lc_out, c).start()

        return carry

    @pl.when(lc_send & first)
    def _():
        pl.semaphore_wait(rdy_lc, 1)
        for c in range(NCH):
            lc_copy(ab_ref, c).start()

    @pl.when((z == ends[0]) & carry)
    def _():
        pl.semaphore_wait(rdy_pc, 1)
        for c in range(NCH):
            pc_copy(ab_ref, c).start()

    @pl.when(opens)
    def _():
        pl.semaphore_wait(rdy_pc, 1)
        for c in range(HALF, NCH):
            pc_copy(ab_ref, c).start()

    @pl.when(late)
    def _():
        pl.semaphore_wait(rdy_b0, 1)
        b0_copy().start()

    @pl.when(lc_recv)
    def _():
        set_rhs(rhs, ab_ref)

        @pl.when(lc_send)
        def _():
            pl.semaphore_wait(rdy_lc, 1)

        lax.fori_loop(0, HALF, lc_step, 0)

        @pl.when(lc_send | (z == last))
        def _():
            lax.fori_loop(HALF, NCH, lc_step, 0)

    def pc_step(c, carry):
        pc_copy(ab_ref, c).wait_recv()
        for p in range(prompts):
            y = dot(left3(pc_in[c, p]), rhs2[p])
            pc_out[c, p] = y + jnp.where(c >= HALF, comp[c, p], 0.0)

        @pl.when(pc_send)
        def _():
            pc_copy(pc_out, c).start()

        return carry

    @pl.when(pc_recv)
    def _():
        @pl.when(first)
        def _():
            for c in range(NCH):
                comp[c] = ab_ref[c]

        set_rhs(rhs2, comp)

        @pl.when(pc_send)
        def _():
            pl.semaphore_wait(rdy_pc, 1)

        @pl.when(carry)
        def _():
            lax.fori_loop(0, HALF, pc_step, 0)

        @pl.when(lc_recv & (z != last))
        def _():
            lax.fori_loop(HALF, NCH, lc_step, 0)

        @pl.when((z == last) & carry)
        def _():
            set_rhs(rhs, pc_out)
            b0_copy().wait_recv()
            for p in range(prompts):
                start = jnp.concatenate([b0_in[c, p] for c in range(HALF)], axis=0)
                fin = dot(left3(start), rhs[p])
                for c in range(HALF):
                    comp[HALF + c, p] = comp[HALF + c, p] + fin[c * CH : (c + 1) * CH]

        lax.fori_loop(HALF, NCH, pc_step, 0)

    tile_per = CH // 8

    def st_copy(zz):
        t = zz // 2
        return pltpu.make_async_remote_copy(
            src_ref=pc_out.at[HALF + t // tile_per, :, pl.ds((t % tile_per) * 8, 8), :], dst_ref=st_in, send_sem=st_ss, recv_sem=st_rs, device_id=dev(zz), device_id_type=MESH
        )

    def nm_copy():
        return pltpu.make_async_remote_copy(
            src_ref=nm_out, dst_ref=nm_in, send_sem=nm_ss, recv_sem=nm_rs, device_id=dev(1), device_id_type=MESH
        )

    order = []
    for k in range(n):
        for zz in (k, last - 1 - k):
            if zz not in order and 0 <= zz < last:
                order.append(zz)

    @pl.when(z == last)
    def _():
        query = q_ref[...].astype(F32)
        query = query * lax.rsqrt(jnp.sum(query * query, axis=-1, keepdims=True) + EPS) * DK**-0.5
        reads = []
        for p in range(prompts):
            fin = jnp.concatenate([pc_out[HALF + c, p] for c in range(HALF)], axis=0)
            qh, ql = split(jnp.broadcast_to(query[p : p + 1], (8, DK)))
            fh, fl = split(fin)
            read = lax.dot_general(
                jnp.concatenate([qh, ql, qh], axis=1), jnp.concatenate([fh, fh, fl], axis=1), NT, preferred_element_type=F32
            )
            reads.append(read[0:1])
        read = jnp.concatenate(reads, axis=0)
        scaled = read * lax.rsqrt(jnp.mean(read * read, axis=-1, keepdims=True) + EPS)
        gate = gate_ref[...].astype(F32)
        normed = (scaled * gain_ref[...] * (gate * jax.nn.sigmoid(gate))).astype(BF16)
        nm_out[...] = normed.astype(F32)
        nm_copy().start()
        for zz in order:
            st_copy(zz).start()
        t = last // 2
        for p in range(prompts):
            st_in[p] = pc_out[HALF + t // tile_per, p, (t % tile_per) * 8 : (t % tile_per) * 8 + 8, :]

    def pt_copy(k):
        return pltpu.make_async_remote_copy(
            src_ref=part.at[tp], dst_ref=part.at[tp], send_sem=pt_ss, recv_sem=pt_rs, device_id=dev(1, lax.rem(tp + k, ntp)), device_id_type=MESH
        )

    def pt_all():
        some = part.at[pl.ds(0, ntp - 1)]
        return pltpu.make_async_remote_copy(
            src_ref=some, dst_ref=some, send_sem=pt_ss, recv_sem=pt_rs, device_id=dev(0), device_id_type=MESH
        )

    def p0_all():
        return pltpu.make_async_remote_copy(
            src_ref=part0, dst_ref=part0, send_sem=p0_ss, recv_sem=p0_rs, device_id=dev(last), device_id_type=MESH
        )

    def p0_copy(k):
        return pltpu.make_async_remote_copy(
            src_ref=part.at[tp, 0], dst_ref=part0.at[tp], send_sem=p0_ss, recv_sem=p0_rs, device_id=dev(0, lax.rem(tp + k, ntp)), device_id_type=MESH
        )

    def fin_copy(zz):
        return pltpu.make_async_remote_copy(
            src_ref=tot.at[zz // 2], dst_ref=fin_in, send_sem=fn_ss, recv_sem=fn_rs, device_id=dev(zz), device_id_type=MESH
        )

    out_order = [zz for k in range(1, n) for zz in (1 + k, (1 - k) % n) if 1 < zz < n]
    out_order = [zz for i, zz in enumerate(out_order) if zz not in out_order[:i]]

    @pl.when(z == 1)
    def _():
        pltpu.make_async_remote_copy(
            src_ref=ow_all.at[pl.ds(0, n - 1)], dst_ref=ow_all.at[pl.ds(0, n - 1)], send_sem=ow_ss, recv_sem=ow_rs, device_id=dev(0), device_id_type=MESH
        ).wait_recv()
        lines = ow_all.shape[1]
        for r in range(lines):
            ow_mat[pl.ds(r * n, n), :] = ow_all[:, r, :].astype(BF16)
        vr = lax.broadcasted_iota(jnp.int32, (DK, DK), 0)
        vc = lax.broadcasted_iota(jnp.int32, (DK, DK), 1)
        perm = jnp.where(vc == (vr % lines) * n + vr // lines, 1.0, 0.0).astype(BF16)
        half = ow_mat.shape[1] // 4
        for h in range(4):
            ow_mat[:, pl.ds(h * half, half)] = dot(perm, ow_mat[:, pl.ds(h * half, half)]).astype(BF16)
        pl.semaphore_wait(rdy_p0, ntp)
        nm_copy().wait_recv()
        lhs = jnp.concatenate([nm_in[...], jnp.zeros((8 - prompts, DK), F32)], axis=0).astype(BF16)
        part[tp, 0] = dot(lhs, ow_mat[:, 0:128])[0:prompts]
        for k in range(ntp):
            p0_copy(k).start()
        res = dot(lhs, ow_mat[:, 128:])
        for t in range(1, tiles):
            part[tp, t] = res[0:prompts, (t - 1) * 128 : t * 128]
        for k in range(1, ntp):
            pt_copy(k).start()
        pt_all().wait_recv()
        acc = part[0]
        for k in range(1, ntp):
            acc = acc + part[k]
        tot[...] = acc
        for zz in out_order:
            fin_copy(zz).start()
        fin_in[...] = acc[0]

    @pl.when(z != last)
    def _():
        pltpu.make_async_remote_copy(
            src_ref=st_in, dst_ref=st_in, send_sem=st_ss, recv_sem=st_rs, device_id=dev(last), device_id_type=MESH
        ).wait_recv()

    odd = lax.rem(z, 2)
    for p in range(prompts):
        st_ref[p] = jnp.where(odd == 1, st_in[p, 4:8, :], st_in[p, 0:4, :]).astype(BF16)

    @pl.when(z > 1)
    def _():
        pltpu.make_async_remote_copy(
            src_ref=fin_in, dst_ref=fin_in, send_sem=fn_ss, recv_sem=fn_rs, device_id=dev(1), device_id_type=MESH
        ).wait_recv()

    @pl.when(z == 0)
    def _():
        p0_all().wait_recv()
        acc = part0[0]
        for k in range(1, ntp):
            acc = acc + part0[k]
        fin_in[...] = acc

    at = odd * (ntp * span) + tp * span
    value = fin_in[...]
    lane = lax.broadcasted_iota(jnp.int32, (128, span), 0)
    want = lax.broadcasted_iota(jnp.int32, (128, span), 1) + at
    v1, v2 = split(value)
    v3 = (value - v1.astype(F32) - v2.astype(F32)).astype(BF16)
    sel = jnp.where(lane == want, 1.0, 0.0).astype(BF16)
    ro_ref[...] = dot(jnp.concatenate([v1, v2, v3], axis=1), jnp.concatenate([sel, sel, sel], axis=0))

    @pl.when(z != 1)
    def _():
        ow_copy().wait_send()

    @pl.when(lc_send)
    def _():
        pltpu.make_async_remote_copy(
            src_ref=lc_out, dst_ref=lc_in, send_sem=lc_ss, recv_sem=lc_rs.at[0], device_id=dev(z + 1), device_id_type=MESH
        ).wait_send()

    def pc_sent(rows):
        pltpu.make_async_remote_copy(
            src_ref=pc_out.at[rows], dst_ref=pc_in.at[rows], send_sem=pc_ss, recv_sem=pc_rs.at[0], device_id=dev(next_head), device_id_type=MESH
        ).wait_send()

    @pl.when(pc_send & carry)
    def _():
        pc_sent(pl.ds(0, NCH))

    @pl.when(pc_send & jnp.logical_not(carry))
    def _():
        pc_sent(pl.ds(HALF, HALF))

    @pl.when(late)
    def _():
        b0_copy().wait_send()

    @pl.when(z == last)
    def _():
        pltpu.make_async_remote_copy(
            src_ref=st_size, dst_ref=st_size, send_sem=st_ss, recv_sem=st_rs, device_id=dev(0), device_id_type=MESH
        ).wait_send()
        nm_copy().wait_send()

    @pl.when(z == 1)
    def _():
        pt_all().wait_send()
        p0_all().wait_send()
        pltpu.make_async_remote_copy(
            src_ref=fn_size, dst_ref=fn_size, send_sem=fn_ss, recv_sem=fn_rs, device_id=dev(0), device_id_type=MESH
        ).wait_send()


VM = pl.BlockSpec(memory_space=pltpu.VMEM)
ANY = pl.BlockSpec(memory_space=pl.ANY)


def fused(n, ntp, x, wk, wv, bw, shift, dw, rate, extra, q, gate, gain, ow):
    prompts, seg, width = x.shape
    total = prompts * seg
    groups = total // BLK
    chunks = total // ROWS
    lines = ow.shape[1]
    sizes = GROUPS if n == sum(GROUPS) + 1 else (1,) * (n - 1)
    span = ow.shape[2] // (n * ntp)
    tiles = ow.shape[2] // 128
    vm = pltpu.VMEM
    blk = vm((NCH, prompts, CH, DK), F32)
    dma = pltpu.SemaphoreType.DMA
    reg = pltpu.SemaphoreType.REGULAR
    square = vm((groups, BLK, BLK), F32)
    small = [vm(a.shape, a.dtype) for a in (bw, shift, dw, rate, extra, q, gate, gain, ow)]
    return pl.pallas_call(
        functools.partial(body, n, ntp, sizes),
        name="delta_states",
        out_shape=(
            pltpu.VMEM((prompts, lines, DK), BF16),
            pltpu.VMEM((prompts, span), F32),
        ),
        in_specs=[ANY] * 12,
        out_specs=(VM, VM),
        scratch_shapes=[
            vm((width, 2 * DK), BF16),
            vm((total, width), BF16),
            vm((total, 2 * DK), BF16),
            square, square, square,
            *small,
            blk, blk, blk, blk, blk, blk,
            vm((prompts, 3 * DK, DK), BF16),
            vm((prompts, 3 * DK, DK), BF16),
            vm((HALF, prompts, CH, DK), F32),
            vm((prompts, 8, DK), F32),
            vm((prompts, 8, DK), F32),
            vm((prompts, DK), F32),
            vm((prompts, DK), F32),
            vm((lines, ow.shape[2]), F32),
            vm((n, lines, ow.shape[2]), F32),
            vm((n * lines, ow.shape[2]), BF16),
            vm((ntp, tiles, prompts, 128), F32),
            vm((ntp, prompts, 128), F32),
            vm((tiles, prompts, 128), F32),
            vm((prompts, 128), F32),
            vm((n - 1, prompts, 8, DK), F32),
            vm((n - 2, prompts, 128), F32),
            dma((chunks,)), dma((4,)), dma((7,)),
            dma, dma((NCH,)), dma, dma((NCH,)),
            dma, dma,
            dma, dma,
            dma, dma,
            dma, dma,
            dma, dma,
            dma, dma,
            dma, dma,
            reg, reg, reg, reg,
        ],
        compiler_params=pltpu.CompilerParams(collective_id=0, has_side_effects=True),
    )(x, wk, wv, bw, shift, dw, rate, extra, q, gate, gain, ow)


def hand_over(st_in, ro_in, st_out, ro_out, sem):
    copies = [pltpu.make_async_copy(st_in, st_out, sem.at[0]), pltpu.make_async_copy(ro_in, ro_out, sem.at[1])]
    for c in copies:
        c.start()
    for c in copies:
        c.wait()


def finish(st, ro):
    return pl.pallas_call(
        hand_over,
        name="hand_over",
        out_shape=(jax.ShapeDtypeStruct(st.shape, st.dtype), jax.ShapeDtypeStruct(ro.shape, ro.dtype)),
        in_specs=[ANY, ANY],
        out_specs=(ANY, ANY),
        scratch_shapes=[pltpu.SemaphoreType.DMA((2,))],
        compiler_params=pltpu.CompilerParams(vmem_limit_bytes=1024 * 1024),
    )(st, ro)


def solution(mesh):
    n, ntp = mesh.shape["sp"], mesh.shape["tp"]

    def per_device(x, wk, wv, bw, shift, dw, rate, extra, q, gate, gain, ow):
        prompts, seg, width = x.shape
        st, ro = fused(n, ntp, x, wk, wv, bw.T, shift.reshape(1, -1), dw.T, rate.reshape(1, -1), extra.reshape(prompts, 1, seg), q, gate, gain.reshape(1, -1), ow)
        st, ro = finish(st, ro)
        return jnp.transpose(st, (0, 2, 1))[:, None], ro

    placed = (
        P("grp", "sp", None),
        P(None, "tp"),
        P(None, "tp"),
        P(),
        P(),
        P(),
        P(),
        P("grp", "sp", "tp"),
        P("grp", "tp"),
        P("grp", "tp"),
        P(),
        P("tp", "sp", None),
    )
    return jax.shard_map(
        per_device,
        mesh=mesh,
        in_specs=placed,
        out_specs=(P("grp", "tp", None, "sp"), P("grp", ("sp", "tp"))),
        check_vma=False,
    )
```

```python
import functools

import jax
import jax.numpy as jnp
from jax import lax
from jax.experimental import pallas as pl
from jax.experimental.pallas import tpu as pltpu
from jax.sharding import PartitionSpec as P

MESH = pl.DeviceIdType.MESH
EPS = 1e-06
F32 = jnp.float32
BF16 = jnp.bfloat16
DK = 128
BLK = 128
CH = 16
ROWS = 256
HALF = DK // CH
NCH = 2 * HALF
GROUPS = (1, 1, 1, 1, 1, 2, 2, 2, 2, 2, 2, 2, 3, 4, 5)
NT = (((1,), (1,)), ((), ()))


def dot(a, b):
    return jnp.dot(a, b, preferred_element_type=F32)


def split(a):
    high = a.astype(BF16)
    return high, (a - high.astype(F32)).astype(BF16)


def left3(a):
    high, low = split(a)
    return jnp.concatenate([high, low, high], axis=1)


def right3(b):
    high, low = split(b)
    return jnp.concatenate([high, high, low], axis=0)


def left2(a):
    return jnp.concatenate(split(a), axis=1)


def dot3(a, b):
    return dot(left3(a), right3(b))


def local_body(middle, tp, prompts, seg, wcopies, copies, scopies, bw_ref, dw_ref, shift_ref, rate_ref, extra_ref, ab_ref, w_buf, x_buf, kv_buf, m_buf, t_buf, y_buf):
    rows = ROWS
    chunks = len(copies)
    for c in wcopies:
        c.wait()
    for c in copies[1:]:
        c.start()
    wbd = jnp.concatenate([bw_ref[...], dw_ref[...]], axis=0)
    raw = []
    for j in range(chunks):
        copies[j].wait()
        xs = x_buf[pl.ds(j * rows, rows), :]
        kv_buf[pl.ds(j * rows, rows), :] = dot(xs, w_buf[...]).astype(BF16)
        raw.append(lax.dot_general(wbd, xs, NT, preferred_element_type=F32))
    middle()
    for c in scopies:
        c.wait()
    groups = prompts * seg // BLK
    gp = seg // BLK
    heads = bw_ref.shape[0]
    head_lane = lax.broadcasted_iota(jnp.int32, (2 * heads, 1), 0)
    pick_b = head_lane == tp
    pick_d = head_lane == tp + heads

    def pack(pick):
        lines = []
        for g in range(groups):
            at = g * BLK
            block = raw[at // rows][:, at % rows : at % rows + BLK]
            lines.append(jnp.sum(jnp.where(pick, block, 0.0), axis=0, keepdims=True))
        return jnp.concatenate(lines, axis=0)

    beta_raw = pack(pick_b).astype(BF16).astype(F32)
    decay_raw = pack(pick_d).astype(BF16).astype(F32)
    extra = jnp.concatenate(
        [extra_ref[g // gp, :, pl.ds((g % gp) * BLK, BLK)] for g in range(groups)], axis=0
    )
    own = lax.broadcasted_iota(jnp.int32, (1, heads), 1) == tp
    shift = jnp.sum(jnp.where(own, shift_ref[...], 0.0), axis=1, keepdims=True)
    rate = jnp.sum(jnp.where(own, rate_ref[...], 0.0), axis=1, keepdims=True)
    beta = jax.nn.sigmoid(beta_raw + shift)
    softplus = jnp.maximum(decay_raw, 0.0) + jnp.log1p(jnp.exp(-jnp.abs(decay_raw)))
    log_decay = -rate * softplus + extra
    row = lax.broadcasted_iota(jnp.int32, (BLK, BLK), 0)
    col = lax.broadcasted_iota(jnp.int32, (BLK, BLK), 1)
    upto = jnp.where(row <= col, 1.0, 0.0).astype(BF16)
    l1 = log_decay.astype(BF16)
    l2 = (log_decay - l1.astype(F32)).astype(BF16)
    l3 = (log_decay - l1.astype(F32) - l2.astype(F32)).astype(BF16)
    cum = dot(jnp.concatenate([l1, l2, l3], axis=1), jnp.concatenate([upto, upto, upto], axis=0))
    cum_t = cum.T
    beta_t = beta.T
    eye = row == col
    upper = row < col
    ident = jnp.where(eye, 1.0, 0.0)
    neu = upper & ((row >> 3) == (col >> 3))
    norms = []
    for g in range(groups):
        k = kv_buf[pl.ds(g * BLK, BLK), pl.ds(0, DK)]
        gram = lax.dot_general(k, k, NT, preferred_element_type=F32)
        diag = jnp.where(eye, gram, 0.0)
        r_row = lax.rsqrt(jnp.sum(diag, axis=0, keepdims=True) + EPS)
        r_col = lax.rsqrt(jnp.sum(diag, axis=1, keepdims=True) + EPS)
        c_row = cum[g : g + 1, :]
        c_col = cum_t[:, g : g + 1]
        scale = jnp.exp(jnp.where(upper, c_row - c_col, 0.0)) * (beta[g : g + 1, :] * r_row) * r_col
        m = jnp.where(upper, gram * scale, 0.0)
        m_buf[g] = m
        t_buf[g] = jnp.where(neu, m, 0.0)
        norms.append((r_row, r_col))
    p2 = []
    for g in range(groups):
        p = t_buf[g]
        p2.append(dot3(p, p))
    for g in range(groups):
        p = t_buf[g]
        both = dot3(p2[g], jnp.concatenate([p2[g], p], axis=1))
        y_buf[g] = both[:, :BLK]
        t_buf[g] = ident - p + p2[g] - both[:, BLK:]
    for g in range(groups):
        q = t_buf[g]
        t_buf[g] = q + dot3(q, y_buf[g])
    s = 8
    while s < BLK:
        mask = ((row // (2 * s)) == (col // (2 * s))) & ((row // s) % 2 == 0) & ((col // s) % 2 == 1)
        for g in range(groups):
            y_buf[g] = dot3(jnp.where(mask, m_buf[g], 0.0), t_buf[g])
        for g in range(groups):
            t = t_buf[g]
            t_buf[g] = t - dot3(t, y_buf[g])
        s *= 2
    for g in range(groups):
        r_row, r_col = norms[g]
        c_row = cum[g : g + 1, :]
        last = cum[g : g + 1, BLK - 1 : BLK]
        t = t_buf[g] * (jnp.exp(last - c_row) * r_row)
        b_col = beta_t[:, g : g + 1]
        e_col = jnp.exp(cum_t[:, g : g + 1]) * r_col * b_col
        k = kv_buf[pl.ds(g * BLK, BLK), pl.ds(0, DK)]
        v = kv_buf[pl.ds(g * BLK, BLK), pl.ds(DK, DK)]
        k2 = jnp.concatenate([k, k], axis=0)
        f = dot(left2(jnp.concatenate([t * e_col, t * b_col], axis=0)), k2)
        kt = k.T
        vt = v.T
        a_part = dot(jnp.concatenate([kt, kt], axis=1), jnp.concatenate(split(f[:BLK]), axis=0))
        b_part = dot(jnp.concatenate([vt, vt], axis=1), jnp.concatenate(split(f[BLK:]), axis=0))
        y_buf2 = jnp.concatenate([ident * jnp.exp(last) - a_part, b_part], axis=0)
        if g % gp == 0:
            maps = []
        maps.append(y_buf2)
        if g % gp == gp - 1:
            while len(maps) > 1:
                nexts = []
                for a in range(0, len(maps), 2):
                    early, late = maps[a], maps[a + 1]
                    prod = dot3(early, late[:DK])
                    nexts.append(jnp.concatenate([prod[:DK], prod[DK:] + late[DK:]], axis=0))
                maps = nexts
            p = g // gp
            for c in range(NCH):
                ab_ref[c, p] = maps[0][c * CH : (c + 1) * CH]


def body(n, ntp, sizes, x_hbm, wk_hbm, wv_hbm, bw_hbm, shift_hbm, dw_hbm, rate_hbm, extra_hbm, q_hbm, gate_hbm, gain_hbm, ow_hbm, st_ref, ro_ref, w_buf, x_buf, kv_buf, m_buf, t_buf, y_buf, bw_ref, shift_ref, dw_ref, rate_ref, extra_ref, q_ref, gate_ref, gain_ref, ow_ref, ab_ref, lc_in, pc_in, lc_out, pc_out, comp, rhs, rhs2, b0_in, dummy, st_in, nm_out, nm_in, ow_out, ow_all, ow_mat, part, part0, tot, fin_in, st_size, fn_size, x_sem, w_sem, in_sem, lc_ss, lc_rs, pc_ss, pc_rs, b0_ss, b0_rs, st_ss, st_rs, nm_ss, nm_rs, ow_ss, ow_rs, pt_ss, pt_rs, p0_ss, p0_rs, fn_ss, fn_rs, rdy_lc, rdy_pc, rdy_b0, rdy_p0):
    grp = lax.axis_index("grp")
    z = lax.axis_index("sp")
    tp = lax.axis_index("tp")
    last = n - 1
    prompts, seg, width = x_hbm.shape
    tiles = tot.shape[0]
    span = ro_ref.shape[1]

    wcopies = [
        pltpu.make_async_copy(wk_hbm, w_buf.at[:, pl.ds(0, DK)], w_sem.at[0]),
        pltpu.make_async_copy(wv_hbm, w_buf.at[:, pl.ds(DK, DK)], w_sem.at[1]),
    ]
    wcopies += [pltpu.make_async_copy(bw_hbm, bw_ref, w_sem.at[2]), pltpu.make_async_copy(dw_hbm, dw_ref, w_sem.at[3])]
    small = [(shift_hbm, shift_ref), (rate_hbm, rate_ref), (extra_hbm, extra_ref), (q_hbm, q_ref), (gate_hbm, gate_ref), (gain_hbm, gain_ref), (ow_hbm, ow_ref)]
    scopies = [pltpu.make_async_copy(a, b, in_sem.at[i]) for i, (a, b) in enumerate(small)]
    per = seg // ROWS
    copies = []
    for j in range(prompts * per):
        copies.append(
            pltpu.make_async_copy(x_hbm.at[j // per, pl.ds((j % per) * ROWS, ROWS), :], x_buf.at[pl.ds(j * ROWS, ROWS), :], x_sem.at[j])
        )
    for c in wcopies:
        c.start()

    def dev(zz, t=None):
        return (grp, zz, tp if t is None else t)

    ends = []
    at = 0
    for size in sizes:
        at += size
        ends.append(at)
    starts = [e - size + 1 for e, size in zip(ends, sizes)]

    def among(values):
        hit = z == values[0]
        for v in values[1:]:
            hit = hit | (z == v)
        return hit

    def table(keys, values):
        out = jnp.int32(0)
        for k, v in zip(keys, values):
            out = jnp.where(z == k, jnp.int32(v), out)
        return out

    head = among(ends)
    first = among(starts)
    lc_recv = (z >= 1) & jnp.logical_not(first)
    lc_send = (z >= 1) & jnp.logical_not(head)
    carry = tp == 0
    late = (z == 0) & carry
    opens = (z == 0) & jnp.logical_not(carry)
    pc_recv = head & ((z > ends[0]) | jnp.logical_not(carry))
    pc_send = (head & (z < last)) | opens
    prev_head = table(ends[1:], ends[:-1])
    next_head = jnp.where(z == 0, ends[0], table(ends[:-1], ends[1:]))

    bar = pltpu.get_barrier_semaphore()

    @pl.when(z == 1)
    def _():
        for zz in range(2, n):
            pl.semaphore_signal(bar, inc=1, device_id=dev(zz), device_id_type=MESH)
        for k in range(1, ntp):
            pl.semaphore_signal(bar, inc=1, device_id=dev(z, lax.rem(tp + k, ntp)), device_id_type=MESH)
        for k in range(ntp):
            pl.semaphore_signal(bar, inc=1, device_id=dev(0, lax.rem(tp + k, ntp)), device_id_type=MESH)

    @pl.when(lc_send)
    def _():
        pl.semaphore_signal(bar, inc=1, device_id=dev(z + 1), device_id_type=MESH)

    @pl.when(pc_send)
    def _():
        pl.semaphore_signal(bar, inc=1, device_id=dev(next_head), device_id_type=MESH)

    @pl.when(z != last)
    def _():
        pl.semaphore_signal(bar, inc=1, device_id=dev(last), device_id_type=MESH)

    copies[0].start()
    for c in scopies:
        c.start()
    one = jnp.int32(1)
    zero = jnp.int32(0)
    expect = (
        jnp.where(z == 0, ntp, jnp.where(z == 1, ntp - 1, 1))
        + jnp.where(lc_recv, one, zero)
        + jnp.where(pc_recv, one, zero)
        + jnp.where(z == last, n - 1, 0)
    )
    def ow_copy():
        return pltpu.make_async_remote_copy(
            src_ref=ow_out, dst_ref=ow_all.at[z], send_sem=ow_ss, recv_sem=ow_rs, device_id=dev(1), device_id_type=MESH
        )

    def middle():
        scopies[6].wait()
        ow_out[...] = ow_ref[0].astype(F32)
        pl.semaphore_wait(bar, expect)

        @pl.when(lc_recv)
        def _():
            pl.semaphore_signal(rdy_lc, inc=1, device_id=dev(z - 1), device_id_type=MESH)

        @pl.when(pc_recv)
        def _():
            pl.semaphore_signal(rdy_pc, inc=1, device_id=dev(prev_head), device_id_type=MESH)

        @pl.when((z == last) & carry)
        def _():
            pl.semaphore_signal(rdy_b0, inc=1, device_id=dev(0), device_id_type=MESH)

        @pl.when(z == 0)
        def _():
            for k in range(ntp):
                pl.semaphore_signal(rdy_p0, inc=1, device_id=dev(1, lax.rem(tp + k, ntp)), device_id_type=MESH)

        @pl.when(z != 1)
        def _():
            ow_copy().start()

        @pl.when(z == 1)
        def _():
            ow_all[1] = ow_out[...]

    local_body(middle, tp, prompts, seg, wcopies, copies, scopies[:6], bw_ref, dw_ref, shift_ref, rate_ref, extra_ref, ab_ref, w_buf, x_buf, kv_buf, m_buf, t_buf, y_buf)

    def lc_copy(src, c):
        return pltpu.make_async_remote_copy(
            src_ref=src.at[c], dst_ref=lc_in.at[c], send_sem=lc_ss, recv_sem=lc_rs.at[c], device_id=dev(z + 1), device_id_type=MESH
        )

    def pc_copy(src, c):
        return pltpu.make_async_remote_copy(
            src_ref=src.at[c], dst_ref=pc_in.at[c], send_sem=pc_ss, recv_sem=pc_rs.at[c], device_id=dev(next_head), device_id_type=MESH
        )

    def b0_copy():
        return pltpu.make_async_remote_copy(
            src_ref=ab_ref.at[pl.ds(HALF, HALF)], dst_ref=b0_in, send_sem=b0_ss, recv_sem=b0_rs, device_id=dev(last), device_id_type=MESH
        )

    def set_rhs(dst, src):
        for p in range(prompts):
            a = jnp.concatenate([src[c, p] for c in range(HALF)], axis=0)
            dst[p] = right3(a)

    def lc_step(c, carry):
        lc_copy(ab_ref, c).wait_recv()
        for p in range(prompts):
            y = dot(left3(lc_in[c, p]), rhs[p])
            y = y + jnp.where(c >= HALF, ab_ref[c, p], 0.0)
            lc_out[c, p] = y
            comp[c, p] = y

        @pl.when(lc_send)
        def _():
            lc_copy(lc_out, c).start()

        return carry

    @pl.when(lc_send & first)
    def _():
        pl.semaphore_wait(rdy_lc, 1)
        for c in range(NCH):
            lc_copy(ab_ref, c).start()

    @pl.when((z == ends[0]) & carry)
    def _():
        pl.semaphore_wait(rdy_pc, 1)
        for c in range(NCH):
            pc_copy(ab_ref, c).start()

    @pl.when(opens)
    def _():
        pl.semaphore_wait(rdy_pc, 1)
        for c in range(HALF, NCH):
            pc_copy(ab_ref, c).start()

    @pl.when(late)
    def _():
        pl.semaphore_wait(rdy_b0, 1)
        b0_copy().start()

    @pl.when(lc_recv)
    def _():
        set_rhs(rhs, ab_ref)

        @pl.when(lc_send)
        def _():
            pl.semaphore_wait(rdy_lc, 1)

        lax.fori_loop(0, HALF, lc_step, 0)

        @pl.when(lc_send | (z == last))
        def _():
            lax.fori_loop(HALF, NCH, lc_step, 0)

    def pc_step(c, carry):
        pc_copy(ab_ref, c).wait_recv()
        for p in range(prompts):
            y = dot(left3(pc_in[c, p]), rhs2[p])
            pc_out[c, p] = y + jnp.where(c >= HALF, comp[c, p], 0.0)

        @pl.when(pc_send)
        def _():
            pc_copy(pc_out, c).start()

        return carry

    @pl.when(pc_recv)
    def _():
        @pl.when(first)
        def _():
            for c in range(NCH):
                comp[c] = ab_ref[c]

        set_rhs(rhs2, comp)

        @pl.when(pc_send)
        def _():
            pl.semaphore_wait(rdy_pc, 1)

        @pl.when(carry)
        def _():
            lax.fori_loop(0, HALF, pc_step, 0)

        @pl.when(lc_recv & (z != last))
        def _():
            lax.fori_loop(HALF, NCH, lc_step, 0)

        @pl.when((z == last) & carry)
        def _():
            set_rhs(rhs, pc_out)
            b0_copy().wait_recv()
            for p in range(prompts):
                start = jnp.concatenate([b0_in[c, p] for c in range(HALF)], axis=0)
                fin = dot(left3(start), rhs[p])
                for c in range(HALF):
                    comp[HALF + c, p] = comp[HALF + c, p] + fin[c * CH : (c + 1) * CH]

        lax.fori_loop(HALF, NCH, pc_step, 0)

    tile_per = CH // 8

    def st_copy(zz):
        t = zz // 2
        return pltpu.make_async_remote_copy(
            src_ref=pc_out.at[HALF + t // tile_per, :, pl.ds((t % tile_per) * 8, 8), :], dst_ref=st_in, send_sem=st_ss, recv_sem=st_rs, device_id=dev(zz), device_id_type=MESH
        )

    def nm_copy():
        return pltpu.make_async_remote_copy(
            src_ref=nm_out, dst_ref=nm_in, send_sem=nm_ss, recv_sem=nm_rs, device_id=dev(1), device_id_type=MESH
        )

    order = []
    for k in range(n):
        for zz in (k, last - 1 - k):
            if zz not in order and 0 <= zz < last:
                order.append(zz)

    @pl.when(z == last)
    def _():
        query = q_ref[...].astype(F32)
        query = query * lax.rsqrt(jnp.sum(query * query, axis=-1, keepdims=True) + EPS) * DK**-0.5
        reads = []
        for p in range(prompts):
            fin = jnp.concatenate([pc_out[HALF + c, p] for c in range(HALF)], axis=0)
            qh, ql = split(jnp.broadcast_to(query[p : p + 1], (8, DK)))
            fh, fl = split(fin)
            read = lax.dot_general(
                jnp.concatenate([qh, ql, qh], axis=1), jnp.concatenate([fh, fh, fl], axis=1), NT, preferred_element_type=F32
            )
            reads.append(read[0:1])
        read = jnp.concatenate(reads, axis=0)
        scaled = read * lax.rsqrt(jnp.mean(read * read, axis=-1, keepdims=True) + EPS)
        gate = gate_ref[...].astype(F32)
        normed = (scaled * gain_ref[...] * (gate * jax.nn.sigmoid(gate))).astype(BF16)
        nm_out[...] = normed.astype(F32)
        nm_copy().start()
        for zz in order:
            st_copy(zz).start()
        t = last // 2
        for p in range(prompts):
            st_in[p] = pc_out[HALF + t // tile_per, p, (t % tile_per) * 8 : (t % tile_per) * 8 + 8, :]

    def pt_copy(k):
        return pltpu.make_async_remote_copy(
            src_ref=part.at[tp], dst_ref=part.at[tp], send_sem=pt_ss, recv_sem=pt_rs, device_id=dev(1, lax.rem(tp + k, ntp)), device_id_type=MESH
        )

    def pt_all():
        some = part.at[pl.ds(0, ntp - 1)]
        return pltpu.make_async_remote_copy(
            src_ref=some, dst_ref=some, send_sem=pt_ss, recv_sem=pt_rs, device_id=dev(0), device_id_type=MESH
        )

    def p0_all():
        return pltpu.make_async_remote_copy(
            src_ref=part0, dst_ref=part0, send_sem=p0_ss, recv_sem=p0_rs, device_id=dev(last), device_id_type=MESH
        )

    def p0_copy(k):
        return pltpu.make_async_remote_copy(
            src_ref=part.at[tp, 0], dst_ref=part0.at[tp], send_sem=p0_ss, recv_sem=p0_rs, device_id=dev(0, lax.rem(tp + k, ntp)), device_id_type=MESH
        )

    def fin_copy(zz):
        return pltpu.make_async_remote_copy(
            src_ref=tot.at[zz // 2], dst_ref=fin_in, send_sem=fn_ss, recv_sem=fn_rs, device_id=dev(zz), device_id_type=MESH
        )

    out_order = [zz for k in range(1, n) for zz in (1 + k, (1 - k) % n) if 1 < zz < n]
    out_order = [zz for i, zz in enumerate(out_order) if zz not in out_order[:i]]

    @pl.when(z == 1)
    def _():
        pltpu.make_async_remote_copy(
            src_ref=ow_all.at[pl.ds(0, n - 1)], dst_ref=ow_all.at[pl.ds(0, n - 1)], send_sem=ow_ss, recv_sem=ow_rs, device_id=dev(0), device_id_type=MESH
        ).wait_recv()
        lines = ow_all.shape[1]
        for r in range(lines):
            ow_mat[pl.ds(r * n, n), :] = ow_all[:, r, :].astype(BF16)
        vr = lax.broadcasted_iota(jnp.int32, (DK, DK), 0)
        vc = lax.broadcasted_iota(jnp.int32, (DK, DK), 1)
        perm = jnp.where(vc == (vr % lines) * n + vr // lines, 1.0, 0.0).astype(BF16)
        half = ow_mat.shape[1] // 4
        for h in range(4):
            ow_mat[:, pl.ds(h * half, half)] = dot(perm, ow_mat[:, pl.ds(h * half, half)]).astype(BF16)
        pl.semaphore_wait(rdy_p0, ntp)
        nm_copy().wait_recv()
        lhs = jnp.concatenate([nm_in[...], jnp.zeros((8 - prompts, DK), F32)], axis=0).astype(BF16)
        part[tp, 0] = dot(lhs, ow_mat[:, 0:128])[0:prompts]
        for k in range(ntp):
            p0_copy(k).start()
        res = dot(lhs, ow_mat[:, 128:])
        for t in range(1, tiles):
            part[tp, t] = res[0:prompts, (t - 1) * 128 : t * 128]
        for k in range(1, ntp):
            pt_copy(k).start()
        pt_all().wait_recv()
        acc = part[0]
        for k in range(1, ntp):
            acc = acc + part[k]
        tot[...] = acc
        for zz in out_order:
            fin_copy(zz).start()
        fin_in[...] = acc[0]

    @pl.when(z != last)
    def _():
        pltpu.make_async_remote_copy(
            src_ref=st_in, dst_ref=st_in, send_sem=st_ss, recv_sem=st_rs, device_id=dev(last), device_id_type=MESH
        ).wait_recv()

    odd = lax.rem(z, 2)
    for p in range(prompts):
        st_ref[p] = jnp.where(odd == 1, st_in[p, 4:8, :], st_in[p, 0:4, :]).astype(BF16)

    @pl.when(z > 1)
    def _():
        pltpu.make_async_remote_copy(
            src_ref=fin_in, dst_ref=fin_in, send_sem=fn_ss, recv_sem=fn_rs, device_id=dev(1), device_id_type=MESH
        ).wait_recv()

    @pl.when(z == 0)
    def _():
        p0_all().wait_recv()
        acc = part0[0]
        for k in range(1, ntp):
            acc = acc + part0[k]
        fin_in[...] = acc

    at = odd * (ntp * span) + tp * span
    value = fin_in[...]
    lane = lax.broadcasted_iota(jnp.int32, (128, span), 0)
    want = lax.broadcasted_iota(jnp.int32, (128, span), 1) + at
    v1, v2 = split(value)
    v3 = (value - v1.astype(F32) - v2.astype(F32)).astype(BF16)
    sel = jnp.where(lane == want, 1.0, 0.0).astype(BF16)
    ro_ref[...] = dot(jnp.concatenate([v1, v2, v3], axis=1), jnp.concatenate([sel, sel, sel], axis=0))

    @pl.when(z != 1)
    def _():
        ow_copy().wait_send()

    @pl.when(lc_send)
    def _():
        pltpu.make_async_remote_copy(
            src_ref=lc_out, dst_ref=lc_in, send_sem=lc_ss, recv_sem=lc_rs.at[0], device_id=dev(z + 1), device_id_type=MESH
        ).wait_send()

    def pc_sent(rows):
        pltpu.make_async_remote_copy(
            src_ref=pc_out.at[rows], dst_ref=pc_in.at[rows], send_sem=pc_ss, recv_sem=pc_rs.at[0], device_id=dev(next_head), device_id_type=MESH
        ).wait_send()

    @pl.when(pc_send & carry)
    def _():
        pc_sent(pl.ds(0, NCH))

    @pl.when(pc_send & jnp.logical_not(carry))
    def _():
        pc_sent(pl.ds(HALF, HALF))

    @pl.when(late)
    def _():
        b0_copy().wait_send()

    @pl.when(z == last)
    def _():
        pltpu.make_async_remote_copy(
            src_ref=st_size, dst_ref=st_size, send_sem=st_ss, recv_sem=st_rs, device_id=dev(0), device_id_type=MESH
        ).wait_send()
        nm_copy().wait_send()

    @pl.when(z == 1)
    def _():
        pt_all().wait_send()
        p0_all().wait_send()
        pltpu.make_async_remote_copy(
            src_ref=fn_size, dst_ref=fn_size, send_sem=fn_ss, recv_sem=fn_rs, device_id=dev(0), device_id_type=MESH
        ).wait_send()


VM = pl.BlockSpec(memory_space=pltpu.VMEM)
ANY = pl.BlockSpec(memory_space=pl.ANY)


def fused(n, ntp, x, wk, wv, bw, shift, dw, rate, extra, q, gate, gain, ow):
    prompts, seg, width = x.shape
    total = prompts * seg
    groups = total // BLK
    chunks = total // ROWS
    lines = ow.shape[1]
    sizes = GROUPS if n == sum(GROUPS) + 1 else (1,) * (n - 1)
    span = ow.shape[2] // (n * ntp)
    tiles = ow.shape[2] // 128
    vm = pltpu.VMEM
    blk = vm((NCH, prompts, CH, DK), F32)
    dma = pltpu.SemaphoreType.DMA
    reg = pltpu.SemaphoreType.REGULAR
    square = vm((groups, BLK, BLK), F32)
    small = [vm(a.shape, a.dtype) for a in (bw, shift, dw, rate, extra, q, gate, gain, ow)]
    return pl.pallas_call(
        functools.partial(body, n, ntp, sizes),
        name="delta_states",
        out_shape=(
            pltpu.VMEM((prompts, lines, DK), BF16),
            pltpu.VMEM((prompts, span), F32),
        ),
        in_specs=[ANY] * 12,
        out_specs=(VM, VM),
        scratch_shapes=[
            vm((width, 2 * DK), BF16),
            vm((total, width), BF16),
            vm((total, 2 * DK), BF16),
            square, square, square,
            *small,
            blk, blk, blk, blk, blk, blk,
            vm((prompts, 3 * DK, DK), BF16),
            vm((prompts, 3 * DK, DK), BF16),
            vm((HALF, prompts, CH, DK), F32),
            vm((prompts, 8, DK), F32),
            vm((prompts, 8, DK), F32),
            vm((prompts, DK), F32),
            vm((prompts, DK), F32),
            vm((lines, ow.shape[2]), F32),
            vm((n, lines, ow.shape[2]), F32),
            vm((n * lines, ow.shape[2]), BF16),
            vm((ntp, tiles, prompts, 128), F32),
            vm((ntp, prompts, 128), F32),
            vm((tiles, prompts, 128), F32),
            vm((prompts, 128), F32),
            vm((n - 1, prompts, 8, DK), F32),
            vm((n - 2, prompts, 128), F32),
            dma((chunks,)), dma((4,)), dma((7,)),
            dma, dma((NCH,)), dma, dma((NCH,)),
            dma, dma,
            dma, dma,
            dma, dma,
            dma, dma,
            dma, dma,
            dma, dma,
            dma, dma,
            reg, reg, reg, reg,
        ],
        compiler_params=pltpu.CompilerParams(collective_id=0, has_side_effects=True),
    )(x, wk, wv, bw, shift, dw, rate, extra, q, gate, gain, ow)


def hand_over(st_in, ro_in, st_out, ro_out, sem):
    copies = [pltpu.make_async_copy(st_in, st_out, sem.at[0]), pltpu.make_async_copy(ro_in, ro_out, sem.at[1])]
    for c in copies:
        c.start()
    for c in copies:
        c.wait()


def finish(st, ro):
    return pl.pallas_call(
        hand_over,
        name="hand_over",
        out_shape=(jax.ShapeDtypeStruct(st.shape, st.dtype), jax.ShapeDtypeStruct(ro.shape, ro.dtype)),
        in_specs=[ANY, ANY],
        out_specs=(ANY, ANY),
        scratch_shapes=[pltpu.SemaphoreType.DMA((2,))],
        compiler_params=pltpu.CompilerParams(vmem_limit_bytes=1024 * 1024),
    )(st, ro)


def solution(mesh):
    n, ntp = mesh.shape["sp"], mesh.shape["tp"]

    def per_device(x, wk, wv, bw, shift, dw, rate, extra, q, gate, gain, ow):
        prompts, seg, width = x.shape
        st, ro = fused(n, ntp, x, wk, wv, bw.T, shift.reshape(1, -1), dw.T, rate.reshape(1, -1), extra.reshape(prompts, 1, seg), q, gate, gain.reshape(1, -1), ow)
        st, ro = finish(st, ro)
        return jnp.transpose(st, (0, 2, 1))[:, None], ro

    placed = (
        P("grp", "sp", None),
        P(None, "tp"),
        P(None, "tp"),
        P(),
        P(),
        P(),
        P(),
        P("grp", "sp", "tp"),
        P("grp", "tp"),
        P("grp", "tp"),
        P(),
        P("tp", "sp", None),
    )
    return jax.shard_map(
        per_device,
        mesh=mesh,
        in_specs=placed,
        out_specs=(P("grp", "tp", None, "sp"), P("grp", ("sp", "tp"))),
        check_vma=False,
    )
```
